1024 devices in a mesh: ep: 32 (over z, core), tp: 32 (over y, x).
Axes of the slice: x: 4, y: 8, z: 16, core: 2. Of those that a mesh axis runs over, the one named last changes fastest.
Arguments:
- tokens: bfloat16 [4096, 4096], P('ep', 'tp'), may hold values from -6 to 6
- routes: int32 [4096, 2], P('ep'), may hold values from 0 to 63, all different within a row; in each aligned block of 128 rows (0 to 127, 128 to 255, ...) at most 5 rows name the same one
- route_weights: float32 [4096, 2], P('ep'), may hold values from 0.2 to 2
- cotangent: bfloat16 [4096, 4096], P('ep', 'tp'), may hold values from -6 to 6
- expert_gate: bfloat16 [64, 4096, 512], P('ep', 'tp'), may hold values from -0.09375 to 0.09375
- expert_up: bfloat16 [64, 4096, 512], P('ep', 'tp'), may hold values from -0.09375 to 0.09375
- expert_down: bfloat16 [64, 512, 4096], P('ep', None, 'tp'), may hold values from -0.25 to 0.25
- shared_gate: bfloat16 [4096, 512], P('tp'), may hold values from -0.09375 to 0.09375
- shared_up: bfloat16 [4096, 512], P('tp'), may hold values from -0.09375 to 0.09375
- shared_down: bfloat16 [512, 4096], P(None, 'tp'), may hold values from -0.25 to 0.25
Outputs:
- grad_tokens: bfloat16 [4096, 4096], P('ep', 'tp')
- grad_weights: float32 [4096, 2], P('ep')
- grad_expert_gate: float32 [64, 4096, 512], P('ep', 'tp')
- grad_expert_up: float32 [64, 4096, 512], P('ep', 'tp')
- grad_expert_down: float32 [64, 512, 4096], P('ep', None, 'tp')
- grad_shared_gate: float32 [4096, 512], P('tp', 'ep')
- grad_shared_up: float32 [4096, 512], P('tp', 'ep')
- grad_shared_down: float32 [512, 4096], P('ep', 'tp')
The draws below stay inside these ranges and needn't reach their ends.
Inputs may be any that keep to these rules, and one draw needn't show every extreme that they name: `routes`: each row names 2 different experts. In each aligned block of 128 rows (the rows of one index of ep) no expert is named by more than 5 rows, a bound that some block reaches.
All inputs are finite; a program needn't handle non-finite values.
Results may differ from the reference program's by a relative error of at most 0.0054.
Values may be sent and summed in bfloat16 or wider, within the bound.
No kernel may reach another device: no remote copies, remote signals or barrier semaphores. Data moves between devices by JAX's collectives and lax.ppermute only.
A program may use at most 32 MiB of HBM per device.

```python
import math
import jax
import jax.numpy as jnp
import numpy as np
from jax import lax

D = 4096
FF = 512
SFF = 512
TOPK = 2
TOK_DEV = 128
EXPERTS = 64
CAP = 5
TOKENS = 4096
N_EP = 32


def levels(own_key, shape, cuts, least, largest):
    def one(position, parts):
        heights = jax.random.uniform(jax.random.fold_in(jax.random.fold_in(own_key, 6), position), (parts,), jnp.float32, least / len(cuts), largest / len(cuts))
        return jnp.repeat(jnp.exp(heights), shape[position] // parts).reshape((-1,) + (1,) * (len(shape) - position - 1))

    level = one(*cuts[0])
    for cut in cuts[1:]:
        level = level * one(*cut)
    return level


def routed_block(own_key, own, number, rows, count, top, reach, lean):
    ranking = jax.random.permutation(own_key, count)
    heavy_load, common = portions_of(count, rows * top, reach, lean, True), portions_of(count, rows * top, reach, lean, False)
    places = jnp.arange(count)

    def named(lengths, rotation):
        used = int((lengths > 0).sum())
        fixed = max(1, used // 4)
        shifted = fixed + (places - fixed + rotation * (used - fixed)) % max(1, count - fixed)
        return jnp.zeros((count,), jnp.int32).at[ranking[jnp.where(places < fixed, places, shifted)]].set(jnp.asarray(lengths, jnp.int32))

    lengths = jnp.where(number % 4 == 0, named(heavy_load, number // 4), named(common, number - number // 4 - 1))
    mixed = jax.random.permutation(jax.random.fold_in(own, 3), count)
    giver, sink = mixed[0:count // 2 * 2:2], mixed[1:count // 2 * 2:2]
    margin = jnp.minimum(lengths[giver] - 1, reach - lengths[sink]) // 2
    margin = jnp.where((giver == ranking[0]) | (sink == ranking[0]) | (lengths[sink] == 0), 0, jnp.maximum(margin, 0))
    shifted = jax.random.randint(jax.random.fold_in(own, 4), (count // 2,), 0, 1 << 20) % (margin + 1)
    lengths = lengths.at[giver].add(-shifted).at[sink].add(shifted)
    members = jnp.searchsorted(jnp.cumsum(lengths), jnp.arange(rows * top), side="right").astype(jnp.int32)
    table = members.reshape(top, rows).T
    table = table[jax.random.permutation(jax.random.fold_in(own, 1), rows)]
    rotation = jax.random.randint(jax.random.fold_in(own, 2), (rows, 1), 0, top)
    return jnp.take_along_axis(table, (jnp.arange(top)[None, :] + rotation) % top, axis=1)


def portions_of(number_of, total, most, lean, full):
    loads = [(1 << 20) // math.isqrt(grade ** lean) + 1 for grade in range(1, number_of + 1)]
    largest = most if full else min(most, max(-(-total // number_of), total * loads[0] // sum(loads)))
    least = 1 if total - largest >= number_of - 1 else 0
    given, rest = [largest] + [least] * (number_of - 1), total - largest - least * (number_of - 1)
    while rest > 0:
        free = [i for i in range(1, number_of) if given[i] < largest] or [i for i in range(1, number_of) if given[i] < most]
        pool, remaining = sum([loads[i] for i in free]), rest
        for i in free:
            extra = min(most - given[i], max(1, remaining * loads[i] // pool), rest)
            given[i] = given[i] + extra
            rest = rest - extra
    return np.array(given)


def centred(own_key, dims, width, bound, shards=(), kind=jnp.bfloat16):
    entries = width * jax.random.normal(own_key, dims, jnp.float32)
    if shards:
        entries = entries * levels(own_key, dims, shards, -0.22, 0.18)
    return jnp.clip(entries, -bound, bound).astype(kind)


def setup_inputs(seed: int = 0) -> dict:
    streams_of = jax.random.split(jax.random.key(seed), 11)
    tokens = centred(streams_of[0], (TOKENS, D), 1.0, 6.0, ((0, 32), (1, 32)))
    routes_keys = jax.random.split(jax.random.fold_in(streams_of[1], 1), TOKENS // TOK_DEV)
    routes_turns = jax.random.permutation(jax.random.fold_in(streams_of[1], 3), TOKENS // TOK_DEV)
    routes = jax.vmap(lambda own, number: routed_block(jax.random.fold_in(streams_of[1], 2), own, number, TOK_DEV, EXPERTS, TOPK, CAP, 2))(routes_keys, routes_turns).reshape((TOKENS, TOPK))
    route_weights = jnp.clip(0.2 + 1.8 * jax.random.uniform(streams_of[2], (TOKENS, TOPK), jnp.float32) ** levels(streams_of[2], (TOKENS, TOPK), ((0, 32),), -0.2, 0.2), 0.2, 2.0)
    cotangent = centred(streams_of[3], (TOKENS, D), 1.0, 6.0, ((0, 32), (1, 32)))
    expert_gate = centred(streams_of[4], (EXPERTS, D, FF), D ** -0.5, 0.09375, ((0, 32), (1, 32)))
    expert_up = centred(streams_of[5], (EXPERTS, D, FF), D ** -0.5, 0.09375, ((0, 32), (1, 32)))
    expert_down = centred(streams_of[6], (EXPERTS, FF, D), FF ** -0.5, 0.25, ((0, 32), (2, 32)))
    shared_gate = centred(streams_of[7], (D, SFF), D ** -0.5, 0.09375, ((0, 32),))
    shared_up = centred(streams_of[8], (D, SFF), D ** -0.5, 0.09375, ((0, 32),))
    shared_down = centred(streams_of[9], (SFF, D), SFF ** -0.5, 0.25, ((1, 32),))
    return dict(tokens=tokens, routes=routes, route_weights=route_weights, cotangent=cotangent, expert_gate=expert_gate, expert_up=expert_up, expert_down=expert_down, shared_gate=shared_gate, shared_up=shared_up, shared_down=shared_down)


def rounded(values):
    return lax.optimization_barrier(values.astype(jnp.bfloat16)).astype(jnp.float32)


def hidden_terms(gate_pre, up_pre, back_grad, scaling):
    logistic = jax.nn.sigmoid(gate_pre)
    product = gate_pre * logistic * up_pre
    grad_act = scaling * back_grad
    gate_grad = (grad_act * up_pre * logistic * (1.0 + gate_pre * (1.0 - logistic))).astype(jnp.bfloat16)
    up_grad = (grad_act * gate_pre * logistic).astype(jnp.bfloat16)
    hidden = (scaling * product).astype(jnp.bfloat16)
    return gate_grad, up_grad, hidden, jnp.sum(back_grad * product, axis=-1)


def reference(tokens, routes, route_weights, cotangent, expert_gate, expert_up, expert_down,
              shared_gate, shared_up, shared_down):
    picked = routes.reshape(N_EP, TOK_DEV * TOPK)
    onehot = (picked[:, :, None] == jnp.arange(EXPERTS, dtype=jnp.int32)[None, None, :]).astype(jnp.int32)
    ranked = jnp.sum(jnp.cumsum(onehot, axis=1) * onehot, axis=2) - 1
    block_ids = jnp.arange(N_EP, dtype=jnp.int32)[:, None]
    slot_ids = (picked * (N_EP * CAP) + block_ids * CAP + ranked).reshape(-1).astype(jnp.int32)
    source_ids = jnp.full((EXPERTS * N_EP * CAP,), TOKENS * TOPK, jnp.int32)
    source_ids = source_ids.at[slot_ids].set(jnp.arange(TOKENS * TOPK, dtype=jnp.int32))
    token_ids = (source_ids // TOPK).astype(jnp.int32)
    tokens_pad = jnp.concatenate([tokens, jnp.zeros((1, D), jnp.bfloat16)], axis=0)
    cot_pad = jnp.concatenate([cotangent, jnp.zeros((1, D), jnp.bfloat16)], axis=0)
    gates_pad = jnp.concatenate([rounded(route_weights).reshape(-1), jnp.zeros((1,), jnp.float32)], axis=0)

    def expert_pass(inputs):
        token_index, source_index, weight_gate, weight_up, weight_down = inputs
        slot_tokens = tokens_pad[token_index]
        slot_cotan = cot_pad[token_index]
        slot_gates = gates_pad[source_index]
        gate_pre = jnp.dot(slot_tokens, weight_gate, preferred_element_type=jnp.float32)
        up_pre = jnp.dot(slot_tokens, weight_up, preferred_element_type=jnp.float32)
        back_grad = jnp.dot(slot_cotan, weight_down.T, preferred_element_type=jnp.float32)
        gate_grad, up_grad, hidden, slot_dg = hidden_terms(gate_pre, up_pre, back_grad, slot_gates[:, None])
        slot_grad = (jnp.dot(gate_grad, weight_gate.T, preferred_element_type=jnp.float32)
                     + jnp.dot(up_grad, weight_up.T, preferred_element_type=jnp.float32))
        grad_gate = jnp.dot(slot_tokens.T, gate_grad, preferred_element_type=jnp.float32)
        grad_up = jnp.dot(slot_tokens.T, up_grad, preferred_element_type=jnp.float32)
        grad_down = jnp.dot(hidden.T, slot_cotan, preferred_element_type=jnp.float32)
        return slot_grad, slot_dg, grad_gate, grad_up, grad_down

    slot_grad, slot_dg, grad_expert_gate, grad_expert_up, grad_expert_down = lax.map(
        expert_pass,
        (token_ids.reshape(EXPERTS, N_EP * CAP), source_ids.reshape(EXPERTS, N_EP * CAP),
         expert_gate, expert_up, expert_down))
    routed_grad = slot_grad.reshape(-1, D)[slot_ids].reshape(TOKENS, TOPK, D)
    routed_grad = jnp.sum(routed_grad, axis=1)
    grad_weights = slot_dg.reshape(-1)[slot_ids].reshape(TOKENS, TOPK)

    shared_gate_pre = jnp.dot(tokens, shared_gate, preferred_element_type=jnp.float32)
    shared_up_pre = jnp.dot(tokens, shared_up, preferred_element_type=jnp.float32)
    shared_back = jnp.dot(cotangent, shared_down.T, preferred_element_type=jnp.float32)
    shared_gate_grad, shared_up_grad, shared_hidden, unused_sum = hidden_terms(
        shared_gate_pre, shared_up_pre, shared_back, 1.0)
    shared_grad = (jnp.dot(shared_gate_grad, shared_gate.T, preferred_element_type=jnp.float32)
                   + jnp.dot(shared_up_grad, shared_up.T, preferred_element_type=jnp.float32))
    grad_shared_gate = jnp.dot(tokens.T, shared_gate_grad, preferred_element_type=jnp.float32)
    grad_shared_up = jnp.dot(tokens.T, shared_up_grad, preferred_element_type=jnp.float32)
    grad_shared_down = jnp.dot(shared_hidden.T, cotangent, preferred_element_type=jnp.float32)
    grad_tokens = (routed_grad + shared_grad).astype(jnp.bfloat16)
    return (grad_tokens, grad_weights, grad_expert_gate, grad_expert_up, grad_expert_down,
            grad_shared_gate, grad_shared_up, grad_shared_down)
```

```python
import jax
import jax.numpy as jnp
from jax import lax
from jax.experimental import pallas as pl
from jax.experimental.pallas import tpu as pltpu
from jax.sharding import Mesh
from jax.sharding import PartitionSpec as P

BF, F32, I32 = jnp.bfloat16, jnp.float32, jnp.int32
NZ, NC, NY, NX = 16, 2, 8, 4
NEP, NTP = NZ * NC, NY * NX
CAP, BLK = 5, 16
SLOTS = 2 * CAP
SHR = 4
USED = SLOTS + SHR
XROWS = NY * USED
HID = 512


def iota(shape, dim):
    return lax.broadcasted_iota(I32, shape, dim)


def nn(a, b):
    return jnp.dot(a, b, preferred_element_type=F32)


def nt(a, b):
    return lax.dot_general(a, b, (((1,), (1,)), ((), ())), preferred_element_type=F32)


def tn(a, b):
    return lax.dot_general(a, b, (((0,), (0,)), ((), ())), preferred_element_type=F32)


def onehot(cond):
    return jnp.where(cond, 1.0, 0.0).astype(BF)


def call(kernel, outs):
    def run(*args):
        return pl.pallas_call(
            kernel,
            out_shape=outs,
            in_specs=[pl.BlockSpec(memory_space=pltpu.VMEM)] * len(args),
            out_specs=jax.tree.map(lambda _: pl.BlockSpec(memory_space=pltpu.VMEM), outs),
        )(*args)

    return run


def struct(shape, dtype):
    return jax.ShapeDtypeStruct(shape, dtype)


def route_kernel(routes, weights, tok, cot, send, ids):
    n = tok.shape[0]
    r0, r1 = routes[:, 0:1], routes[:, 1:2]
    lane = iota((n, 128), 1)
    oh0, oh1 = r0 == lane, r1 == lane
    earlier = onehot(iota((n, n), 0) > iota((n, n), 1))
    f0, f1 = jnp.where(oh0, 1.0, 0.0), jnp.where(oh1, 1.0, 0.0)
    c0 = nn(earlier, f0.astype(BF))
    c1 = nn(earlier, f1.astype(BF)) + jnp.sum(f0, axis=0, keepdims=True)
    rank0 = jnp.sum(c0 * f0, axis=1, keepdims=True).astype(I32)
    rank1 = jnp.sum(c1 * f1, axis=1, keepdims=True).astype(I32)
    row0 = (r0 >> 1) * BLK + (r0 & 1) * CAP + rank0
    row1 = (r1 >> 1) * BLK + (r1 & 1) * CAP + rank1
    ids[...] = jnp.where(iota((n, 2), 1) == 0, row0, row1)
    wide = iota((n, NEP * BLK), 1)
    places = onehot((row0 == wide) | (row1 == wide))
    at0 = onehot((row0 >> 4) * BLK + SLOTS == wide)
    at1 = onehot((row1 >> 4) * BLK + SLOTS == wide)
    gates = weights[...].astype(BF).astype(F32)
    lane2 = iota((n, 256), 1)
    g0 = jnp.where(lane2 == (row0 & 15), gates[:, 0:1], 0.0).astype(BF)
    g1 = jnp.where(lane2 == (row1 & 15), gates[:, 1:2], 0.0).astype(BF)
    feats = jnp.concatenate([tok[...], cot[...]], axis=1)
    left = jnp.concatenate([places, at0, at1], axis=0)
    right = jnp.concatenate([feats, g0, g1], axis=0)
    send[...] = tn(left, right).astype(BF)


def partial_kernel(recv, tok, cot, wg, wu, wd, sg, su, sd, out):
    rows = NX * XROWS
    r = iota((rows, 1), 0)
    x = (r * 293) >> 15
    rest = r - x * XROWS
    y = (rest * 293) >> 12
    q = rest - y * USED
    s = y * NX + x
    src = jnp.where(q < SLOTS, s * BLK + q, NEP * BLK + s * SHR + q - SLOTS)
    pick = onehot(src == iota((rows, NEP * BLK + 128), 1))
    feats = jnp.concatenate([tok[...], cot[...]], axis=1)
    data = nn(pick, jnp.concatenate([recv[...], feats], axis=0))
    kinds = (q < CAP, (q >= CAP) & (q < SLOTS), q >= SLOTS)
    t, c = data[:, :128], data[:, 128:]
    tcat = jnp.concatenate([jnp.where(k, t, 0.0).astype(BF) for k in kinds], axis=1)
    ccat = jnp.concatenate([jnp.where(k, c, 0.0).astype(BF) for k in kinds], axis=1)
    wgc = jnp.concatenate([wg[0], wg[1], sg[...]], axis=0)
    out[:, :HID] = nn(tcat, wgc).astype(BF)
    wuc = jnp.concatenate([wu[0], wu[1], su[...]], axis=0)
    out[:, HID : 2 * HID] = nn(tcat, wuc).astype(BF)
    wdc = jnp.concatenate([wd[0], wd[1], sd[...]], axis=1)
    out[:, 2 * HID :] = nt(ccat, wdc).astype(BF)


def middle_kernel(got, out):
    o = iota((NY * BLK, 1), 0)
    q = o & 15
    want = jnp.where(q < USED, (o >> 4) * USED + q, -1)
    r = iota((NY * BLK, XROWS), 1)
    pick = onehot(want == r)
    total = nn(pick, got[0])
    for k in range(1, NX):
        total = total + nn(pick, got[k])
    out[...] = total.astype(BF)


def hidden_kernel(got, recv, out):
    t = lax.axis_index("y") * NX + lax.axis_index("x")
    pre = got[0].astype(F32)
    for k in range(1, NY):
        pre = pre + got[k].astype(F32)
    gate, up, back = pre[:, :HID], pre[:, HID : 2 * HID], pre[:, 2 * HID :]
    q = iota((BLK, 1), 0)
    lane = iota((BLK, 128), 1)
    block = recv[t, :, :128].astype(F32)
    grow = jnp.sum(jnp.where(iota((BLK, 128), 0) == SLOTS, block, 0.0), axis=0, keepdims=True)
    gcol = jnp.sum(jnp.where(lane == iota((BLK, 128), 0), grow, 0.0), axis=1, keepdims=True)
    scale = jnp.where(q < SLOTS, gcol, 1.0)
    logistic = jax.nn.sigmoid(gate)
    product = gate * logistic * up
    grad_act = scale * back
    gate_grad = (grad_act * up * logistic * (1.0 + gate * (1.0 - logistic))).astype(BF)
    up_grad = (grad_act * gate * logistic).astype(BF)
    hidden = (scale * product).astype(BF)
    dg = jnp.sum(back * product, axis=1, keepdims=True)
    lane_h = iota((BLK, HID), 1)
    row_h = iota((BLK, HID), 0)
    line = jnp.sum(jnp.where(lane_h == row_h, dg, 0.0), axis=0, keepdims=True)
    high = line.astype(BF).astype(F32)
    extra = jnp.where(row_h == USED, high, line - high)
    gate_grad = jnp.where(row_h >= USED, extra, gate_grad.astype(F32)).astype(BF)
    for k in range(NY):
        out[k, :, :HID] = gate_grad
        out[k, :, HID : 2 * HID] = up_grad
        out[k, :, 2 * HID :] = hidden


def back_kernel(grads, tok, cot, wg, wu, sg, su, shared_grad, send):
    n = tok.shape[0]
    token = iota((n, 1), 0)
    s = token >> 2
    want = (s & 3) * (NY * BLK) + (s >> 2) * BLK + SLOTS + (token & 3)
    pick = onehot(want == iota((n, NTP * BLK), 1))
    shared = nn(pick, grads[...]).astype(BF)
    shared_grad[...] = nt(shared[:, :HID], sg[...]) + nt(shared[:, HID : 2 * HID], su[...])
    wt = tn(shared[:, : 2 * HID], tok[...]).astype(BF)
    wdn = tn(shared[:, 2 * HID :], cot[...]).astype(BF)
    gg, gu = grads[:, :HID], grads[:, HID : 2 * HID]
    d0 = nt(gg, wg[0]) + nt(gu, wu[0])
    d1 = nt(gg, wg[1]) + nt(gu, wu[1])
    q = iota((NTP * BLK, 1), 0) & 15
    rows = jnp.where(q < CAP, d0, jnp.where(q < SLOTS, d1, gg[:, :128].astype(F32))).astype(BF)
    for y in range(NY):
        for x in range(NX):
            d = y * NX + x
            z, c = d // NC, d % NC
            at = (x * NY + y) * BLK
            send[c, z, 0:BLK] = rows[at : at + BLK]
            send[c, z, BLK : 2 * BLK] = wt[d * BLK : d * BLK + BLK]
            send[c, z, 2 * BLK : 3 * BLK] = wt[HID + d * BLK : HID + d * BLK + BLK]
            send[c, z, 3 * BLK :] = wdn[d * BLK : d * BLK + BLK]


def weights_kernel(grads, recv, og, ou, od):
    blocks = [recv[y * NX + x] for x in range(NX) for y in range(NY)]
    data = jnp.concatenate(blocks, axis=0)
    q = iota((NTP * BLK, 1), 0) & 15
    first = onehot(q < CAP)
    second = onehot((q >= CAP) & (q < SLOTS))
    t, c = data[:, :128], data[:, 128:]
    tcat = jnp.concatenate([t * first, t * second], axis=1)
    ccat = jnp.concatenate([c * first, c * second], axis=1)
    g = tn(tcat, grads[:, :HID])
    og[0], og[1] = g[:128], g[128:]
    u = tn(tcat, grads[:, HID : 2 * HID])
    ou[0], ou[1] = u[:128], u[128:]
    d = tn(grads[:, 2 * HID :], ccat)
    od[0], od[1] = d[:, :128], d[:, 128:]


def core_kernel(got, out):
    for z in range(NZ):
        out[z, :BLK] = got[0, z, :BLK]
        out[z, BLK : 2 * BLK] = got[1, z, :BLK]
        both = got[0, z, BLK:].astype(F32) + got[1, z, BLK:].astype(F32)
        out[z, 2 * BLK :] = both.astype(BF)


def final_kernel(got, ids, shared_grad, grad_tokens, grad_weights, og, ou, od):
    n = ids.shape[0]
    row0, row1 = ids[:, 0:1], ids[:, 1:2]
    back = jnp.concatenate([got[z, : 2 * BLK] for z in range(NZ)], axis=0)
    wide = iota((n, NEP * BLK), 1)
    places = onehot((row0 == wide) | (row1 == wide))
    grad_tokens[...] = (nn(places, back) + shared_grad[...]).astype(BF)
    lane = iota((n, 128), 1)
    sums = []
    for row in (row0, row1):
        base = (row >> 4) * BLK + USED
        line = nn(onehot((wide == base) | (wide == base + 1)), back)
        sums.append(jnp.sum(jnp.where(lane == (row & 15), line, 0.0), axis=1, keepdims=True))
    grad_weights[...] = jnp.where(iota((n, 2), 1) == 0, sums[0], sums[1])
    total = got[0, 2 * BLK :].astype(F32)
    for z in range(1, NZ):
        total = total + got[z, 2 * BLK :].astype(F32)
    od[...] = total[2 * BLK :]
    pad = jnp.zeros((128 - 2 * BLK, 128), F32)
    turned = jnp.concatenate([total[: 2 * BLK], pad], axis=0).T
    og[...] = turned[:, :BLK]
    ou[...] = turned[:, BLK : 2 * BLK]


def swap(array, axis):
    return lax.all_to_all(array, axis, 0, 0, tiled=True)


def body(tok, routes, weights, cot, wg, wu, wd, sg, su, sd):
    n, feats = tok.shape
    send, ids = call(
        route_kernel, (struct((NEP * BLK, 2 * feats), BF), struct((n, 2), I32))
    )(routes, weights, tok, cot)
    recv = swap(send.reshape(NEP, BLK, 2 * feats), ("z", "core"))
    part = call(partial_kernel, struct((NX * XROWS, 3 * HID), BF))(
        recv.reshape(NEP * BLK, 2 * feats), tok, cot, wg, wu, wd, sg, su, sd
    )
    got = swap(part.reshape(NX, XROWS, 3 * HID), "x")
    mid = call(middle_kernel, struct((NY * BLK, 3 * HID), BF))(got)
    got = swap(mid.reshape(NY, BLK, 3 * HID), "y")
    grads = call(hidden_kernel, struct((NY, BLK, 3 * HID), BF))(got, recv)
    grads = swap(grads, "y").reshape(1, NY * BLK, 3 * HID)
    grads = swap(jnp.broadcast_to(grads, (NX, NY * BLK, 3 * HID)), "x")
    grads = grads.reshape(NTP * BLK, 3 * HID)
    shared_grad, back = call(
        back_kernel, (struct((n, feats), F32), struct((NC, NZ, 4 * BLK, feats), BF))
    )(grads, tok, cot, wg, wu, sg, su)
    back = swap(back, "core")
    back = call(core_kernel, struct((NZ, 5 * BLK, feats), BF))(back)
    back = swap(back, "z")
    grad_g, grad_u, grad_d = call(
        weights_kernel,
        (struct((2, feats, HID), F32), struct((2, feats, HID), F32), struct((2, HID, feats), F32)),
    )(grads, recv)
    grad_tokens, grad_weights, shared_g, shared_u, shared_d = call(
        final_kernel,
        (
            struct((n, feats), BF),
            struct((n, 2), F32),
            struct((feats, BLK), F32),
            struct((feats, BLK), F32),
            struct((BLK, feats), F32),
        ),
    )(back, ids, shared_grad)
    return grad_tokens, grad_weights, grad_g, grad_u, grad_d, shared_g, shared_u, shared_d


def solution(mesh):
    ep, tp = ("z", "core"), ("y", "x")
    fine = Mesh(mesh.devices.reshape(NZ, NC, NY, NX), ("z", "core", "y", "x"))
    return jax.shard_map(
        body,
        mesh=fine,
        in_specs=(
            P(ep, tp),
            P(ep, None),
            P(ep, None),
            P(ep, tp),
            P(ep, tp, None),
            P(ep, tp, None),
            P(ep, None, tp),
            P(tp, None),
            P(tp, None),
            P(None, tp),
        ),
        out_specs=(
            P(ep, tp),
            P(ep, None),
            P(ep, tp, None),
            P(ep, tp, None),
            P(ep, None, tp),
            P(tp, ep),
            P(tp, ep),
            P(ep, tp),
        ),
        check_vma=False,
    )
```

```python
import jax
import jax.numpy as jnp
from jax import lax
from jax.experimental import pallas as pl
from jax.experimental.pallas import tpu as pltpu
from jax.sharding import Mesh
from jax.sharding import PartitionSpec as P

BF, F32, I32 = jnp.bfloat16, jnp.float32, jnp.int32
NZ, NC, NY, NX = 16, 2, 8, 4
NEP, NTP = NZ * NC, NY * NX
CAP, BLK = 5, 16
SLOTS = 2 * CAP
SHR = 4
USED = SLOTS + SHR
HID = 512
SCALE_X, SCALE_Y = 256.0, 64.0


def iota(shape, dim):
    return lax.broadcasted_iota(I32, shape, dim)


def nn(a, b):
    return jnp.dot(a, b, preferred_element_type=F32)


def nt(a, b):
    return lax.dot_general(a, b, (((1,), (1,)), ((), ())), preferred_element_type=F32)


def tn(a, b):
    return lax.dot_general(a, b, (((0,), (0,)), ((), ())), preferred_element_type=F32)


def onehot(cond):
    return jnp.where(cond, 1.0, 0.0).astype(BF)


def call(kernel, outs):
    def place(o):
        return o if isinstance(o, jax.ShapeDtypeStruct) else pltpu.VMEM(*o)

    outs = [place(o) for o in outs]

    def run(*args):
        return pl.pallas_call(
            kernel,
            out_shape=outs,
            in_specs=[pl.BlockSpec(memory_space=pltpu.VMEM)] * len(args),
            out_specs=[pl.BlockSpec(memory_space=pltpu.VMEM)] * len(outs),
            compiler_params=pltpu.CompilerParams(vmem_limit_bytes=16 << 20),
        )(*[pltpu.with_memory_space_constraint(a, pltpu.VMEM) for a in args])

    return run


def struct(shape, dtype):
    return jax.ShapeDtypeStruct(shape, dtype)


def route_kernel(routes, weights, tok, cot, send, ids):
    n = tok.shape[0]
    r0, r1 = routes[0:1, :], routes[1:2, :]
    names = iota((NEP * 2, n), 0)
    f0, f1 = jnp.where(r0 == names, 1.0, 0.0), jnp.where(r1 == names, 1.0, 0.0)
    earlier = onehot(iota((n, n), 0) < iota((n, n), 1))
    c0 = nn(f0.astype(BF), earlier)
    c1 = nn(f1.astype(BF), earlier) + jnp.sum(f0, axis=1, keepdims=True)
    rank0 = jnp.sum(c0 * f0, axis=0, keepdims=True).astype(I32)
    rank1 = jnp.sum(c1 * f1, axis=0, keepdims=True).astype(I32)
    row0 = (r0 >> 1) * BLK + (r0 & 1) * CAP + rank0
    row1 = (r1 >> 1) * BLK + (r1 & 1) * CAP + rank1
    ids[0:1, :] = row0
    ids[1:2, :] = row1
    tall = iota((NEP * BLK, n), 0)
    places = onehot((row0 == tall) | (row1 == tall))
    send[:, 128:] = nn(places, cot[...]).astype(BF)
    gates = weights[...].astype(BF).astype(F32)
    data = nn(places, tok[...])
    lane = iota((n, n), 0)
    for row, k in ((row0, 0), (row1, 1)):
        at = jnp.where((row >> 4) * BLK + SLOTS == tall, gates[k : k + 1, :], 0.0).astype(BF)
        data = data + nt(at, onehot(lane == (row & 15)))
    send[:, :128] = data.astype(BF)


def partial_kernel(recv, tok, cot, wg, wu, wd, sg, su, sd, out):
    r = iota((NTP * BLK, 1), 0)
    q = r & 15
    s = ((r >> 4) & (NY - 1)) * NX + (r >> 7)
    src = jnp.where(q < SLOTS, s * BLK + q, NEP * BLK + s * SHR + q - SLOTS)
    src = jnp.where(q < USED, src, -1)
    pick = onehot(src == iota((NTP * BLK, NEP * BLK + 128), 1))
    feats = jnp.concatenate([tok[...], cot[...]], axis=1)
    data = nn(pick, jnp.concatenate([recv[...], feats], axis=0))
    kinds = (q < CAP, (q >= CAP) & (q < SLOTS), q >= SLOTS)
    t, c = data[:, :128], data[:, 128:]
    tcat = jnp.concatenate([jnp.where(k, t, 0.0).astype(BF) for k in kinds], axis=1)
    ccat = jnp.concatenate([jnp.where(k, c, 0.0).astype(BF) for k in kinds], axis=1)
    wgc = jnp.concatenate([wg[0], wg[1], sg[...]], axis=0)
    out[:, :HID] = nn(tcat, wgc) * SCALE_X
    wuc = jnp.concatenate([wu[0], wu[1], su[...]], axis=0)
    out[:, HID : 2 * HID] = nn(tcat, wuc) * SCALE_X
    wdc = jnp.concatenate([wd[0], wd[1], sd[...]], axis=1)
    out[:, 2 * HID :] = nt(ccat, wdc) * SCALE_X


def hidden_kernel(got, recv, out):
    t = lax.axis_index("y") * NX + lax.axis_index("x")
    pre = got[...] * (1.0 / SCALE_Y)
    gate, up, back = pre[:, :HID], pre[:, HID : 2 * HID], pre[:, 2 * HID :]
    q = iota((BLK, 1), 0)
    lane = iota((BLK, 128), 1)
    block = recv[t, :, :128].astype(F32)
    grow = jnp.sum(jnp.where(iota((BLK, 128), 0) == SLOTS, block, 0.0), axis=0, keepdims=True)
    gcol = jnp.sum(jnp.where(lane == iota((BLK, 128), 0), grow, 0.0), axis=1, keepdims=True)
    scale = jnp.where(q < SLOTS, gcol, 1.0)
    logistic = jax.nn.sigmoid(gate)
    product = gate * logistic * up
    grad_act = scale * back
    gate_grad = (grad_act * up * logistic * (1.0 + gate * (1.0 - logistic))).astype(BF)
    up_grad = (grad_act * gate * logistic).astype(BF)
    hidden = (scale * product).astype(BF)
    dg = jnp.sum(back * product, axis=1, keepdims=True)
    lane_h = iota((BLK, HID), 1)
    row_h = iota((BLK, HID), 0)
    line = jnp.sum(jnp.where(lane_h == row_h, dg, 0.0), axis=0, keepdims=True)
    high = line.astype(BF).astype(F32)
    extra = jnp.where(row_h == USED, high, line - high)
    gate_grad = jnp.where(row_h >= USED, extra, gate_grad.astype(F32)).astype(BF)
    for k in range(NY):
        out[k, :, :HID] = gate_grad
        out[k, :, HID : 2 * HID] = up_grad
        out[k, :, 2 * HID :] = hidden


def back_kernel(grads, tok, cot, wg, wu, sg, su, shared_grad, send):
    n = tok.shape[0]
    token = iota((n, 1), 0)
    s = token >> 2
    want = (s & 3) * (NY * BLK) + (s >> 2) * BLK + SLOTS + (token & 3)
    pick = onehot(want == iota((n, NTP * BLK), 1))
    shared = nn(pick, grads[...]).astype(BF)
    shared_grad[...] = nt(shared[:, :HID], sg[...]) + nt(shared[:, HID : 2 * HID], su[...])
    wt = tn(shared[:, : 2 * HID], tok[...]).astype(BF)
    wdn = tn(shared[:, 2 * HID :], cot[...]).astype(BF)
    gg, gu = grads[:, :HID], grads[:, HID : 2 * HID]
    d0 = nt(gg, wg[0]) + nt(gu, wu[0])
    d1 = nt(gg, wg[1]) + nt(gu, wu[1])
    q = iota((NTP * BLK, 1), 0) & 15
    rows = jnp.where(q < CAP, d0, jnp.where(q < SLOTS, d1, gg[:, :128].astype(F32))).astype(BF)
    for y in range(NY):
        for x in range(NX):
            d = y * NX + x
            z, c = d // NC, d % NC
            at = (x * NY + y) * BLK
            send[c, z, 0:BLK] = rows[at : at + BLK]
            send[c, z, BLK : 2 * BLK] = wt[d * BLK : d * BLK + BLK]
            send[c, z, 2 * BLK : 3 * BLK] = wt[HID + d * BLK : HID + d * BLK + BLK]
            send[c, z, 3 * BLK :] = wdn[d * BLK : d * BLK + BLK]


def weights_kernel(grads, recv, og, ou, od):
    blocks = [recv[y * NX + x] for x in range(NX) for y in range(NY)]
    data = jnp.concatenate(blocks, axis=0)
    q = iota((NTP * BLK, 1), 0) & 15
    first = onehot(q < CAP)
    second = onehot((q >= CAP) & (q < SLOTS))
    t, c = data[:, :128], data[:, 128:]
    tcat = jnp.concatenate([t * first, t * second], axis=1)
    ccat = jnp.concatenate([c * first, c * second], axis=1)
    g = tn(tcat, grads[:, :HID])
    og[0], og[1] = g[:128], g[128:]
    u = tn(tcat, grads[:, HID : 2 * HID])
    ou[0], ou[1] = u[:128], u[128:]
    d = tn(grads[:, 2 * HID :], ccat)
    od[0], od[1] = d[:, :128], d[:, 128:]


def core_kernel(got, out):
    for z in range(NZ):
        out[z, :BLK] = got[0, z, :BLK]
        out[z, BLK : 2 * BLK] = got[1, z, :BLK]
        both = got[0, z, BLK:].astype(F32) + got[1, z, BLK:].astype(F32)
        out[z, 2 * BLK :] = both.astype(BF)


def final_kernel(got, ids, shared_grad, grad_tokens, grad_weights, og, ou, od):
    n = ids.shape[1]
    row0, row1 = ids[0:1, :], ids[1:2, :]
    back = jnp.concatenate([got[z, : 2 * BLK] for z in range(NZ)], axis=0)
    tall = iota((NEP * BLK, n), 0)
    places = onehot((row0 == tall) | (row1 == tall))
    grad_tokens[...] = (tn(places, back) + shared_grad[...]).astype(BF)
    lane = iota((n, n), 0)
    for row, k in ((row0, 0), (row1, 1)):
        base = (row >> 4) * BLK + USED
        line = tn(back, onehot((tall == base) | (tall == base + 1)))
        grad_weights[k : k + 1, :] = jnp.sum(
            jnp.where(lane == (row & 15), line, 0.0), axis=0, keepdims=True
        )
    total = got[0, 2 * BLK :].astype(F32)
    for z in range(1, NZ):
        total = total + got[z, 2 * BLK :].astype(F32)
    og[...] = total[:BLK]
    ou[...] = total[BLK : 2 * BLK]
    od[...] = total[2 * BLK :]


def swap(array, axis):
    return lax.all_to_all(array, axis, 0, 0, tiled=True)


def body(tok, routes, weights, cot, wg, wu, wd, sg, su, sd):
    n, feats = tok.shape
    wide = 3 * HID
    send, ids = call(route_kernel, [((NEP * BLK, 2 * feats), BF), ((2, n), I32)])(
        routes.T, weights.T, tok, cot
    )
    recv = swap(send.reshape(NEP, BLK, 2 * feats), ("z", "core"))
    (part,) = call(partial_kernel, [((NTP * BLK, wide), F32)])(
        recv.reshape(NEP * BLK, 2 * feats), tok, cot, wg, wu, wd, sg, su, sd
    )
    got = swap(part.astype(jnp.float16).reshape(NX, NY * BLK, wide), "x")
    mid = jnp.sum(got.astype(F32), axis=0) * (SCALE_Y / SCALE_X)
    got = swap(mid.astype(jnp.float16).reshape(NY, BLK, wide), "y")
    pre = jnp.sum(got.astype(F32), axis=0)
    (grads,) = call(hidden_kernel, [((NY, BLK, wide), BF)])(pre, recv)
    grads = swap(grads, "y").reshape(1, NY * BLK, wide)
    grads = swap(jnp.broadcast_to(grads, (NX, NY * BLK, wide)), "x")
    grads = grads.reshape(NTP * BLK, wide)
    shared_grad, back = call(
        back_kernel, [((n, feats), F32), ((NC, NZ, 4 * BLK, feats), BF)]
    )(grads, tok, cot, wg, wu, sg, su)
    back = swap(back, "core")
    (back,) = call(core_kernel, [((NZ, 5 * BLK, feats), BF)])(back)
    back = swap(back, "z")
    grad_g, grad_u, grad_d = call(
        weights_kernel,
        [struct((2, feats, HID), F32), struct((2, feats, HID), F32), struct((2, HID, feats), F32)],
    )(grads, recv)
    grad_tokens, grad_weights, shared_g, shared_u, shared_d = call(
        final_kernel,
        [
            struct((n, feats), BF),
            struct((2, n), F32),
            struct((BLK, feats), F32),
            struct((BLK, feats), F32),
            struct((BLK, feats), F32),
        ],
    )(back, ids, shared_grad)
    return grad_tokens, grad_weights.T, grad_g, grad_u, grad_d, shared_g.T, shared_u.T, shared_d


def solution(mesh):
    ep, tp = ("z", "core"), ("y", "x")
    fine = Mesh(mesh.devices.reshape(NZ, NC, NY, NX), ("z", "core", "y", "x"))
    return jax.shard_map(
        body,
        mesh=fine,
        in_specs=(
            P(ep, tp),
            P(ep, None),
            P(ep, None),
            P(ep, tp),
            P(ep, tp, None),
            P(ep, tp, None),
            P(ep, None, tp),
            P(tp, None),
            P(tp, None),
            P(None, tp),
        ),
        out_specs=(
            P(ep, tp),
            P(ep, None),
            P(ep, tp, None),
            P(ep, tp, None),
            P(ep, None, tp),
            P(tp, ep),
            P(tp, ep),
            P(ep, tp),
        ),
        check_vma=False,
    )
```

```python
import jax
import jax.numpy as jnp
from jax import lax
from jax.experimental import pallas as pl
from jax.experimental.pallas import tpu as pltpu
from jax.sharding import Mesh
from jax.sharding import PartitionSpec as P

BF, F32, I32 = jnp.bfloat16, jnp.float32, jnp.int32
NZ, NC, NY, NX = 16, 2, 8, 4
NEP, NTP = NZ * NC, NY * NX
CAP, BLK = 5, 16
SLOTS = 2 * CAP
SHR = 4
USED = SLOTS + SHR
HID = 512
SCALE_X, SCALE_Y = 256.0, 64.0

SHIFTS = (1, 3, 2)


def iota(shape, dim):
    return lax.broadcasted_iota(I32, shape, dim)


def nn(a, b):
    return jnp.dot(a, b, preferred_element_type=F32)


def nt(a, b):
    return lax.dot_general(a, b, (((1,), (1,)), ((), ())), preferred_element_type=F32)


def tn(a, b):
    return lax.dot_general(a, b, (((0,), (0,)), ((), ())), preferred_element_type=F32)


def onehot(cond):
    return jnp.where(cond, 1.0, 0.0).astype(BF)


def call(kernel, outs, space=pltpu.VMEM, scratch=()):
    def place(o):
        return o if isinstance(o, jax.ShapeDtypeStruct) else pltpu.VMEM(*o)

    outs = [place(o) for o in outs]

    def run(*args):
        return pl.pallas_call(
            kernel,
            out_shape=outs,
            in_specs=[pl.BlockSpec(memory_space=space)] * len(args),
            out_specs=[pl.BlockSpec(memory_space=pltpu.VMEM)] * len(outs),
            scratch_shapes=scratch,
            compiler_params=pltpu.CompilerParams(vmem_limit_bytes=16 << 20),
        )(*[pltpu.with_memory_space_constraint(a, space) for a in args])

    return run


def struct(shape, dtype):
    return jax.ShapeDtypeStruct(shape, dtype)


def route_kernel(*refs):
    sources, (send, ids), kept = refs[:10], refs[10:12], refs[12:20]
    routes, weights, sems = refs[20:]
    tok, cot = kept[:2]
    copies = [
        pltpu.make_async_copy(a, b, sems.at[k])
        for k, (a, b) in enumerate(zip(sources, (routes, weights, *kept)))
    ]
    for copy in copies:
        copy.start()
    for copy in copies[:4]:
        copy.wait()
    n = tok.shape[0]
    r0, r1 = routes[0:1, :], routes[1:2, :]
    names = iota((NEP * 2, n), 0)
    f0, f1 = jnp.where(r0 == names, 1.0, 0.0), jnp.where(r1 == names, 1.0, 0.0)
    earlier = onehot(iota((n, n), 0) < iota((n, n), 1))
    c0 = nn(f0.astype(BF), earlier)
    c1 = nn(f1.astype(BF), earlier) + jnp.sum(f0, axis=1, keepdims=True)
    rank0 = jnp.sum(c0 * f0, axis=0, keepdims=True).astype(I32)
    rank1 = jnp.sum(c1 * f1, axis=0, keepdims=True).astype(I32)
    row0 = (r0 >> 1) * BLK + (r0 & 1) * CAP + rank0
    row1 = (r1 >> 1) * BLK + (r1 & 1) * CAP + rank1
    ids[0:1, :] = row0
    ids[1:2, :] = row1
    tall = iota((NEP * BLK, n), 0)
    places = onehot((row0 == tall) | (row1 == tall))
    send[:, 128:] = nn(places, cot[...]).astype(BF)
    gates = weights[...].astype(BF).astype(F32)
    data = nn(places, tok[...])
    lane = iota((n, n), 0)
    for row, k in ((row0, 0), (row1, 1)):
        at = jnp.where((row >> 4) * BLK + SLOTS == tall, gates[k : k + 1, :], 0.0).astype(BF)
        data = data + nt(at, onehot(lane == (row & 15)))
    send[:, :128] = data.astype(BF)
    for copy in copies[4:]:
        copy.wait()


def partial_kernel(recv, tok, cot, wg, wu, wd, sg, su, sd, *outs):
    r = iota((NTP * BLK, 1), 0)
    q = r & 15
    s = ((r >> 4) & (NY - 1)) * NX + (((r >> 7) + lax.axis_index("x")) & (NX - 1))
    src = jnp.where(q < SLOTS, s * BLK + q, NEP * BLK + s * SHR + q - SLOTS)
    src = jnp.where(q < USED, src, -1)
    pick = onehot(src == iota((NTP * BLK, NEP * BLK + 128), 1))
    feats = jnp.concatenate([tok[...], cot[...]], axis=1)
    data = nn(pick, jnp.concatenate([recv[...], feats], axis=0))
    kinds = (q < CAP, (q >= CAP) & (q < SLOTS), q >= SLOTS)
    t, c = data[:, :128], data[:, 128:]
    tcat = jnp.concatenate([jnp.where(k, t, 0.0).astype(BF) for k in kinds], axis=1)
    ccat = jnp.concatenate([jnp.where(k, c, 0.0).astype(BF) for k in kinds], axis=1)
    wgc = jnp.concatenate([wg[0], wg[1], sg[...]], axis=0)
    wuc = jnp.concatenate([wu[0], wu[1], su[...]], axis=0)
    wdc = jnp.concatenate([wd[0], wd[1], sd[...]], axis=1)
    parts = (nn(tcat, wgc), nn(tcat, wuc), nt(ccat, wdc))
    for k in range(NX):
        for j, part in enumerate(parts):
            outs[k][:, j * HID : j * HID + HID] = part[k * 128 : k * 128 + 128] * SCALE_X


def hidden_kernel(got, recv, out):
    t = lax.axis_index("y") * NX + lax.axis_index("x")
    pre = got[...] * (1.0 / SCALE_Y)
    gate, up, back = pre[:, :HID], pre[:, HID : 2 * HID], pre[:, 2 * HID :]
    q = iota((BLK, 1), 0)
    lane = iota((BLK, 128), 1)
    block = recv[t, :, :128].astype(F32)
    grow = jnp.sum(jnp.where(iota((BLK, 128), 0) == SLOTS, block, 0.0), axis=0, keepdims=True)
    gcol = jnp.sum(jnp.where(lane == iota((BLK, 128), 0), grow, 0.0), axis=1, keepdims=True)
    scale = jnp.where(q < SLOTS, gcol, 1.0)
    logistic = jax.nn.sigmoid(gate)
    product = gate * logistic * up
    grad_act = scale * back
    gate_grad = (grad_act * up * logistic * (1.0 + gate * (1.0 - logistic))).astype(BF)
    up_grad = (grad_act * gate * logistic).astype(BF)
    hidden = (scale * product).astype(BF)
    dg = jnp.sum(back * product, axis=1, keepdims=True)
    lane_h = iota((BLK, HID), 1)
    row_h = iota((BLK, HID), 0)
    line = jnp.sum(jnp.where(lane_h == row_h, dg, 0.0), axis=0, keepdims=True)
    high = line.astype(BF).astype(F32)
    extra = jnp.where(row_h == USED, high, line - high)
    gate_grad = jnp.where(row_h >= USED, extra, gate_grad.astype(F32)).astype(BF)
    for k in range(NY):
        out[k, :, :HID] = gate_grad
        out[k, :, HID : 2 * HID] = up_grad
        out[k, :, 2 * HID :] = hidden


def back_kernel(g0, g1, g2, g3, tok, cot, wg, wu, sg, su, shared_grad, send):
    n = tok.shape[0]
    me = lax.axis_index("x")
    grads = jnp.concatenate([g0[...], g1[...], g2[...], g3[...]], axis=0)
    token = iota((n, 1), 0)
    s = token >> 2
    turn = (me - s) & (NX - 1)
    want = turn * (NY * BLK) + (s >> 2) * BLK + SLOTS + (token & 3)
    pick = onehot(want == iota((n, NTP * BLK), 1))
    shared = nn(pick, grads).astype(BF)
    shared_grad[...] = nt(shared[:, :HID], sg[...]) + nt(shared[:, HID : 2 * HID], su[...])
    wt = tn(shared[:, : 2 * HID], tok[...]).astype(BF)
    wdn = tn(shared[:, 2 * HID :], cot[...]).astype(BF)
    gg, gu = grads[:, :HID], grads[:, HID : 2 * HID]
    d0 = nt(gg, wg[0]) + nt(gu, wu[0])
    d1 = nt(gg, wg[1]) + nt(gu, wu[1])
    q = iota((NTP * BLK, 1), 0) & 15
    rows = jnp.where(q < CAP, d0, jnp.where(q < SLOTS, d1, gg[:, :128].astype(F32))).astype(BF)
    for k in range(NX):
        for y in range(NY):
            d = y * NX + ((me - k) & (NX - 1))
            at = (k * NY + y) * BLK
            send[d & 1, d >> 1, 0:BLK] = rows[at : at + BLK]
    for d in range(NEP):
        z, c = d // NC, d % NC
        send[c, z, BLK : 2 * BLK] = wt[d * BLK : d * BLK + BLK]
        send[c, z, 2 * BLK : 3 * BLK] = wt[HID + d * BLK : HID + d * BLK + BLK]
        send[c, z, 3 * BLK :] = wdn[d * BLK : d * BLK + BLK]


def weights_kernel(g0, g1, g2, g3, recv, og, ou, od):
    me = lax.axis_index("x")
    grads = jnp.concatenate([g0[...], g1[...], g2[...], g3[...]], axis=0)
    blocks = [
        recv[y * NX + ((me - k) & (NX - 1))] for k in range(NX) for y in range(NY)
    ]
    data = jnp.concatenate(blocks, axis=0)
    q = iota((NTP * BLK, 1), 0) & 15
    first = onehot(q < CAP)
    second = onehot((q >= CAP) & (q < SLOTS))
    t, c = data[:, :128], data[:, 128:]
    tcat = jnp.concatenate([t * first, t * second], axis=1)
    ccat = jnp.concatenate([c * first, c * second], axis=1)
    g = tn(tcat, grads[:, :HID])
    og[0], og[1] = g[:128], g[128:]
    u = tn(tcat, grads[:, HID : 2 * HID])
    ou[0], ou[1] = u[:128], u[128:]
    d = tn(grads[:, 2 * HID :], ccat)
    od[0], od[1] = d[:, :128], d[:, 128:]


def core_kernel(got, out):
    for z in range(NZ):
        out[z, :BLK] = got[0, z, :BLK]
        out[z, BLK : 2 * BLK] = got[1, z, :BLK]
        both = got[0, z, BLK:].astype(F32) + got[1, z, BLK:].astype(F32)
        out[z, 2 * BLK :] = both.astype(BF)


def final_kernel(got, ids, shared_grad, grad_tokens, grad_weights, og, ou, od):
    n = ids.shape[1]
    row0, row1 = ids[0:1, :], ids[1:2, :]
    back = jnp.concatenate([got[z, : 2 * BLK] for z in range(NZ)], axis=0)
    tall = iota((NEP * BLK, n), 0)
    places = onehot((row0 == tall) | (row1 == tall))
    grad_tokens[...] = (tn(places, back) + shared_grad[...]).astype(BF)
    lane = iota((n, n), 0)
    for row, k in ((row0, 0), (row1, 1)):
        base = (row >> 4) * BLK + USED
        line = tn(back, onehot((tall == base) | (tall == base + 1)))
        grad_weights[k : k + 1, :] = jnp.sum(
            jnp.where(lane == (row & 15), line, 0.0), axis=0, keepdims=True
        )
    total = got[0, 2 * BLK :].astype(F32)
    for z in range(1, NZ):
        total = total + got[z, 2 * BLK :].astype(F32)
    og[...] = total[:BLK]
    ou[...] = total[BLK : 2 * BLK]
    od[...] = total[2 * BLK :]


def swap(array, axis):
    return lax.all_to_all(array, axis, 0, 0, tiled=True)


def turn(array, shift):
    return lax.ppermute(array, "x", [(i, (i + shift) % NX) for i in range(NX)])


def body(tok, routes, weights, cot, wg, wu, wd, sg, su, sd):
    n, feats = tok.shape
    wide = 3 * HID
    params = (tok, cot, wg, wu, wd, sg, su, sd)
    send, ids, *params = call(
        route_kernel,
        [((NEP * BLK, 2 * feats), BF), ((2, n), I32)] + [(p.shape, BF) for p in params],
        space=pltpu.HBM,
        scratch=[
            pltpu.VMEM((2, n), I32),
            pltpu.VMEM((2, n), F32),
            pltpu.SemaphoreType.DMA((10,)),
        ],
    )(routes.T, weights.T, *params)
    tok, cot, wg, wu, wd, sg, su, sd = params
    recv = swap(send.reshape(NEP, BLK, 2 * feats), ("z", "core"))
    parts = call(partial_kernel, [((NY * BLK, wide), F32)] * NX)(
        recv.reshape(NEP * BLK, 2 * feats), *params
    )
    got = [turn(parts[k].astype(jnp.float16), k) for k in SHIFTS]
    mid = sum([g.astype(F32) for g in got], parts[0]) * (SCALE_Y / SCALE_X)
    got = swap(mid.astype(jnp.float16).reshape(NY, BLK, wide), "y")
    pre = jnp.sum(got.astype(F32), axis=0)
    (grads,) = call(hidden_kernel, [((NY, BLK, wide), BF)])(pre, recv)
    own = swap(grads, "y").reshape(NY * BLK, wide)
    turned = {k: turn(own, k) for k in SHIFTS}
    grads = (own, turned[1], turned[2], turned[3])
    shared_grad, back = call(
        back_kernel, [((n, feats), F32), ((NC, NZ, 4 * BLK, feats), BF)]
    )(*grads, tok, cot, wg, wu, sg, su)
    back = swap(back, "core")
    (back,) = call(core_kernel, [((NZ, 5 * BLK, feats), BF)])(back)
    back = swap(back, "z")
    grad_g, grad_u, grad_d = call(
        weights_kernel,
        [struct((2, feats, HID), F32), struct((2, feats, HID), F32), struct((2, HID, feats), F32)],
    )(*grads, recv)
    grad_tokens, grad_weights, shared_g, shared_u, shared_d = call(
        final_kernel,
        [
            struct((n, feats), BF),
            struct((2, n), F32),
            struct((BLK, feats), F32),
            struct((BLK, feats), F32),
            struct((BLK, feats), F32),
        ],
    )(back, ids, shared_grad)
    return grad_tokens, grad_weights.T, grad_g, grad_u, grad_d, shared_g.T, shared_u.T, shared_d


def solution(mesh):
    ep, tp = ("z", "core"), ("y", "x")
    fine = Mesh(mesh.devices.reshape(NZ, NC, NY, NX), ("z", "core", "y", "x"))
    return jax.shard_map(
        body,
        mesh=fine,
        in_specs=(
            P(ep, tp),
            P(ep, None),
            P(ep, None),
            P(ep, tp),
            P(ep, tp, None),
            P(ep, tp, None),
            P(ep, None, tp),
            P(tp, None),
            P(tp, None),
            P(None, tp),
        ),
        out_specs=(
            P(ep, tp),
            P(ep, None),
            P(ep, tp, None),
            P(ep, tp, None),
            P(ep, None, tp),
            P(tp, ep),
            P(tp, ep),
            P(ep, tp),
        ),
        check_vma=False,
    )
```

```python
import jax
import jax.numpy as jnp
from jax import lax
from jax.experimental import pallas as pl
from jax.experimental.pallas import tpu as pltpu
from jax.sharding import Mesh
from jax.sharding import PartitionSpec as P

BF, F16, F32, I32 = jnp.bfloat16, jnp.float16, jnp.float32, jnp.int32
NZ, NC, NY, NX = 16, 2, 8, 4
NEP, NTP = NZ * NC, NY * NX
CAP, BLK = 5, 16
SLOTS = 2 * CAP
SHR = 4
USED = SLOTS + SHR
HID = 512
SCALE_X, SCALE_Y = 256.0, 64.0

SHIFTS = (1, 3, 2)


def iota(shape, dim):
    return lax.broadcasted_iota(I32, shape, dim)


def nn(a, b):
    return jnp.dot(a, b, preferred_element_type=F32)


def nt(a, b):
    return lax.dot_general(a, b, (((1,), (1,)), ((), ())), preferred_element_type=F32)


def tn(a, b):
    return lax.dot_general(a, b, (((0,), (0,)), ((), ())), preferred_element_type=F32)


def onehot(cond):
    return jnp.where(cond, 1.0, 0.0).astype(BF)


def call(kernel, outs, space=pltpu.VMEM, scratch=()):
    def place(o):
        return o if isinstance(o, jax.ShapeDtypeStruct) else pltpu.VMEM(*o)

    outs = [place(o) for o in outs]

    def run(*args):
        return pl.pallas_call(
            kernel,
            out_shape=outs,
            in_specs=[pl.BlockSpec(memory_space=space)] * len(args),
            out_specs=[pl.BlockSpec(memory_space=pltpu.VMEM)] * len(outs),
            scratch_shapes=scratch,
            compiler_params=pltpu.CompilerParams(vmem_limit_bytes=16 << 20),
        )(*[pltpu.with_memory_space_constraint(a, space) for a in args])

    return run


def struct(shape, dtype):
    return jax.ShapeDtypeStruct(shape, dtype)


def route_kernel(*refs):
    sources, (send, ids), kept = refs[:10], refs[10:12], refs[12:20]
    routes, weights, sems = refs[20:]
    tok, cot = kept[:2]
    copies = [
        pltpu.make_async_copy(a, b, sems.at[k])
        for k, (a, b) in enumerate(zip(sources, (routes, weights, *kept)))
    ]
    for copy in copies:
        copy.start()
    for copy in copies[:4]:
        copy.wait()
    n = tok.shape[0]
    r0, r1 = routes[0:1, :], routes[1:2, :]
    names = iota((NEP * 2, n), 0)
    f0, f1 = jnp.where(r0 == names, 1.0, 0.0), jnp.where(r1 == names, 1.0, 0.0)
    earlier = onehot(iota((n, n), 0) < iota((n, n), 1))
    c0 = nn(f0.astype(BF), earlier)
    c1 = nn(f1.astype(BF), earlier) + jnp.sum(f0, axis=1, keepdims=True)
    rank0 = jnp.sum(c0 * f0, axis=0, keepdims=True).astype(I32)
    rank1 = jnp.sum(c1 * f1, axis=0, keepdims=True).astype(I32)
    row0 = (r0 >> 1) * BLK + (r0 & 1) * CAP + rank0
    row1 = (r1 >> 1) * BLK + (r1 & 1) * CAP + rank1
    ids[0:1, :] = row0
    ids[1:2, :] = row1
    tall = iota((NEP * BLK, n), 0)
    places = onehot((row0 == tall) | (row1 == tall))
    send[:, 128:] = nn(places, cot[...]).astype(BF)
    gates = weights[...].astype(BF).astype(F32)
    data = nn(places, tok[...])
    lane = iota((n, n), 0)
    for row, k in ((row0, 0), (row1, 1)):
        at = jnp.where((row >> 4) * BLK + SLOTS == tall, gates[k : k + 1, :], 0.0).astype(BF)
        data = data + nt(at, onehot(lane == (row & 15)))
    send[:, :128] = data.astype(BF)
    for copy in copies[4:]:
        copy.wait()


def split_rows(r, size):
    if size == USED:
        x = (r * 293) >> 15
        rest = r - x * (NY * USED)
        y = (rest * 293) >> 12
    else:
        x = (r * 205) >> 14
        rest = r - x * (NY * SLOTS)
        y = (rest * 205) >> 11
    return x, y, rest - y * size


def shared_kernel(tok, cot, sg, su, sd, *outs):
    me = lax.axis_index("x")
    r = iota((NTP * SHR, 1), 0)
    s = ((r >> 2) & (NY - 1)) * NX + (((r >> 5) + me) & (NX - 1))
    pick = onehot(s * SHR + (r & 3) == iota((NTP * SHR, 128), 1))
    t = nn(pick, tok[...]).astype(BF)
    c = nn(pick, cot[...]).astype(BF)
    rows = NY * SHR
    for j, part in enumerate((nn(t, sg[...]), nn(t, su[...]), nt(c, sd[...]))):
        for k in range(NX):
            outs[k][:, j * HID : j * HID + HID] = part[k * rows : k * rows + rows] * SCALE_X


def partial_kernel(recv, wg, wu, wd, out):
    x, y, q = split_rows(iota((NTP * SLOTS, 1), 0), SLOTS)
    pick = onehot((y * NX + x) * BLK + q == iota((NTP * SLOTS, NEP * BLK), 1))
    data = nn(pick, recv[...])
    t, c = data[:, :128], data[:, 128:]
    kinds = (q < CAP, q >= CAP)
    tcat = jnp.concatenate([jnp.where(k, t, 0.0).astype(BF) for k in kinds], axis=1)
    ccat = jnp.concatenate([jnp.where(k, c, 0.0).astype(BF) for k in kinds], axis=1)
    wgc = jnp.concatenate([wg[0], wg[1]], axis=0)
    wuc = jnp.concatenate([wu[0], wu[1]], axis=0)
    wdc = jnp.concatenate([wd[0], wd[1]], axis=1)
    out[:, :HID] = nn(tcat, wgc) * SCALE_X
    out[:, HID : 2 * HID] = nn(tcat, wuc) * SCALE_X
    out[:, 2 * HID :] = nt(ccat, wdc) * SCALE_X


def merge_kernel(routed, shared, out):
    for y in range(NY):
        at = y * BLK
        out[at : at + SLOTS] = routed[y * SLOTS : y * SLOTS + SLOTS] * (SCALE_Y / SCALE_X)
        out[at + SLOTS : at + USED] = shared[y * SHR : y * SHR + SHR] * (SCALE_Y / SCALE_X)
        out[at + USED : at + BLK] = jnp.zeros((BLK - USED, out.shape[1]), F32)


def hidden_kernel(got, recv, out):
    t = lax.axis_index("y") * NX + lax.axis_index("x")
    pre = got[...] * (1.0 / SCALE_Y)
    gate, up, back = pre[:, :HID], pre[:, HID : 2 * HID], pre[:, 2 * HID :]
    q = iota((BLK, 1), 0)
    lane = iota((BLK, 128), 1)
    block = recv[t, :, :128].astype(F32)
    grow = jnp.sum(jnp.where(iota((BLK, 128), 0) == SLOTS, block, 0.0), axis=0, keepdims=True)
    gcol = jnp.sum(jnp.where(lane == iota((BLK, 128), 0), grow, 0.0), axis=1, keepdims=True)
    scale = jnp.where(q < SLOTS, gcol, 1.0)
    logistic = jax.nn.sigmoid(gate)
    product = gate * logistic * up
    grad_act = scale * back
    gate_grad = (grad_act * up * logistic * (1.0 + gate * (1.0 - logistic))).astype(BF)
    up_grad = (grad_act * gate * logistic).astype(BF)
    hidden = (scale * product).astype(BF)
    dg = jnp.sum(back * product, axis=1, keepdims=True)
    lane_h = iota((BLK, HID), 1)
    row_h = iota((BLK, HID), 0)
    line = jnp.sum(jnp.where(lane_h == row_h, dg, 0.0), axis=0, keepdims=True)
    high = line.astype(BF).astype(F32)
    extra = jnp.where(row_h == USED, high, line - high)
    gate_grad = jnp.where(row_h >= USED, extra, gate_grad.astype(F32)).astype(BF)
    for k in range(NY):
        out[k, :, :HID] = gate_grad
        out[k, :, HID : 2 * HID] = up_grad
        out[k, :, 2 * HID :] = hidden


def pack_kernel(own, main, hid):
    data = own[:, : 2 * HID]
    hidden = own[:, 2 * HID :]
    r = iota((NY * USED, 1), 0)
    _, y, q = split_rows(r, USED)
    grads = nn(onehot(y * BLK + q == iota((NY * USED, NY * BLK), 1)), data).astype(BF)
    j = iota((BLK, 1), 0)
    lane = iota((BLK, NY * BLK), 1)
    left = nn(onehot((j >> 2) * BLK + SLOTS + (j & 3) == lane), hidden)
    right = nn(onehot(((j >> 2) + 4) * BLK + SLOTS + (j & 3) == lane), hidden)
    row = iota((NY, 1), 0) * BLK + USED
    lane = iota((NY, NY * BLK), 1)
    high = nn(onehot(row == lane), data[:, :128])
    low = nn(onehot(row + 1 == lane), data[:, :128])
    rest = jnp.zeros((NY, 2 * HID - 256), F32)
    shared = jnp.concatenate([left, right], axis=1).astype(BF)
    lines = jnp.concatenate([high, low, rest], axis=1).astype(BF)
    for k in range(NX):
        main[k, : NY * USED] = grads
        main[k, NY * USED : NY * BLK] = shared
        main[k, NY * BLK :] = lines
    _, y, q = split_rows(iota((NY * SLOTS, 1), 0), SLOTS)
    hid[...] = nn(onehot(y * BLK + q == iota((NY * SLOTS, NY * BLK), 1)), hidden).astype(BF)


def back_kernel(main, tok, cot, wg, wu, sg, su, shared_grad, send):
    n = tok.shape[0]
    rows, total = NY * USED, NTP * USED
    grads = jnp.concatenate([main[x, :rows] for x in range(NX)], axis=0)
    hidden = jnp.concatenate([main[x, rows : NY * BLK] for x in range(NX)], axis=0)
    lines = jnp.concatenate([main[x, NY * BLK :, :256] for x in range(NX)], axis=0)
    token = iota((n, 1), 0)
    y, x, t = token >> 4, (token >> 2) & 3, token & 3
    pick = onehot(x * rows + y * USED + SLOTS + t == iota((n, total), 1))
    shared = nn(pick, grads).astype(BF)
    j = y * SHR + t
    place = x * BLK + (j & 15)
    lane = iota((n, NX * BLK), 1)
    near = onehot((j < BLK) & (place == lane))
    far = onehot((j >= BLK) & (place == lane))
    shared_hidden = (nn(near, hidden[:, :HID]) + nn(far, hidden[:, HID:])).astype(BF)
    shared_grad[...] = nt(shared[:, :HID], sg[...]) + nt(shared[:, HID:], su[...])
    wt = tn(shared, tok[...]).astype(BF)
    wdn = tn(shared_hidden, cot[...]).astype(BF)
    gg, gu = grads[:, :HID], grads[:, HID:]
    d0 = nt(gg, wg[0]) + nt(gu, wu[0])
    d1 = nt(gg, wg[1]) + nt(gu, wu[1])
    _, _, q = split_rows(iota((total, 1), 0), USED)
    slots = jnp.where(q < CAP, d0, d1).astype(BF)
    o = iota((NEP * BLK, 1), 0)
    q, d = o & 15, o >> 4
    want = jnp.where(q < SLOTS, (d & 3) * rows + (d >> 2) * USED + q, -1)
    back = nn(onehot(want == iota((NEP * BLK, total), 1)), slots)
    source = (d & 3) * NY + (d >> 2)
    lane = iota((NEP * BLK, NTP), 1)
    back = back + nn(onehot((q == USED) & (source == lane)), lines[:, :128])
    back = back + nn(onehot((q == USED + 1) & (source == lane)), lines[:, 128:])
    back = back.astype(BF)
    for d in range(NEP):
        z, c = d // NC, d % NC
        send[c, z, 0:BLK] = back[d * BLK : d * BLK + BLK]
        send[c, z, BLK : 2 * BLK] = wt[d * BLK : d * BLK + BLK]
        send[c, z, 2 * BLK : 3 * BLK] = wt[HID + d * BLK : HID + d * BLK + BLK]
        send[c, z, 3 * BLK :] = wdn[d * BLK : d * BLK + BLK]


def weights_kernel(main, recv, og, ou):
    rows, total = NY * USED, NTP * USED
    grads = jnp.concatenate([main[x, :rows] for x in range(NX)], axis=0)
    x, y, q = split_rows(iota((total, 1), 0), USED)
    place = (y * NX + x) * BLK + q
    lane = iota((total, NEP * BLK), 1)
    data = recv[:, :128]
    t0 = nn(onehot((q < CAP) & (place == lane)), data).astype(BF)
    t1 = nn(onehot((q >= CAP) & (q < SLOTS) & (place == lane)), data).astype(BF)
    tcat = jnp.concatenate([t0, t1], axis=1)
    g = tn(tcat, grads[:, :HID])
    og[0], og[1] = g[:128], g[128:]
    u = tn(tcat, grads[:, HID:])
    ou[0], ou[1] = u[:128], u[128:]


def down_kernel(h0, h1, h2, h3, recv, od):
    me = lax.axis_index("x")
    hidden = jnp.concatenate([h0[...], h1[...], h2[...], h3[...]], axis=0)
    k, y, q = split_rows(iota((NTP * SLOTS, 1), 0), SLOTS)
    place = (y * NX + ((me - k) & (NX - 1))) * BLK + q
    lane = iota((NTP * SLOTS, NEP * BLK), 1)
    data = recv[:, 128:]
    c0 = nn(onehot((q < CAP) & (place == lane)), data).astype(BF)
    c1 = nn(onehot((q >= CAP) & (place == lane)), data).astype(BF)
    d = tn(hidden, jnp.concatenate([c0, c1], axis=1))
    od[0], od[1] = d[:, :128], d[:, 128:]


def core_kernel(got, out):
    for z in range(NZ):
        out[z, :BLK] = got[0, z, :BLK]
        out[z, BLK : 2 * BLK] = got[1, z, :BLK]
        both = got[0, z, BLK:].astype(F32) + got[1, z, BLK:].astype(F32)
        out[z, 2 * BLK :] = both.astype(BF)


def final_kernel(got, ids, shared_grad, grad_tokens, grad_weights, og, ou, od):
    n = ids.shape[1]
    row0, row1 = ids[0:1, :], ids[1:2, :]
    back = jnp.concatenate([got[z, : 2 * BLK] for z in range(NZ)], axis=0)
    tall = iota((NEP * BLK, n), 0)
    places = onehot((row0 == tall) | (row1 == tall))
    grad_tokens[...] = (tn(places, back) + shared_grad[...]).astype(BF)
    lane = iota((n, n), 0)
    for row, k in ((row0, 0), (row1, 1)):
        base = (row >> 4) * BLK + USED
        line = tn(back, onehot((tall == base) | (tall == base + 1)))
        grad_weights[k : k + 1, :] = jnp.sum(
            jnp.where(lane == (row & 15), line, 0.0), axis=0, keepdims=True
        )
    total = got[0, 2 * BLK :].astype(F32)
    for z in range(1, NZ):
        total = total + got[z, 2 * BLK :].astype(F32)
    og[...] = total[:BLK]
    ou[...] = total[BLK : 2 * BLK]
    od[...] = total[2 * BLK :]


def swap(array, axis):
    return lax.all_to_all(array, axis, 0, 0, tiled=True)


def turn(array, shift):
    return lax.ppermute(array, "x", [(i, (i + shift) % NX) for i in range(NX)])


def body(tok, routes, weights, cot, wg, wu, wd, sg, su, sd):
    n, feats = tok.shape
    wide = 3 * HID
    params = (tok, cot, wg, wu, wd, sg, su, sd)
    send, ids, *params = call(
        route_kernel,
        [((NEP * BLK, 2 * feats), BF), ((2, n), I32)] + [(p.shape, BF) for p in params],
        space=pltpu.HBM,
        scratch=[
            pltpu.VMEM((2, n), I32),
            pltpu.VMEM((2, n), F32),
            pltpu.SemaphoreType.DMA((10,)),
        ],
    )(routes.T, weights.T, *params)
    tok, cot, wg, wu, wd, sg, su, sd = params
    recv = swap(send.reshape(NEP, BLK, 2 * feats), ("z", "core"))
    shared = call(shared_kernel, [((NY * SHR, wide), F32)] * NX)(tok, cot, sg, su, sd)
    moved = [turn(shared[k].astype(F16), k).astype(F32) for k in SHIFTS]
    shared = sum(moved, shared[0])
    recv, shared = lax.optimization_barrier((recv, shared))
    flat = recv.reshape(NEP * BLK, 2 * feats)
    (part,) = call(partial_kernel, [((NTP * SLOTS, wide), F32)])(flat, wg, wu, wd)
    got = swap(part.astype(F16).reshape(NX, NY * SLOTS, wide), "x")
    routed = jnp.sum(got.astype(F32), axis=0)
    (mid,) = call(merge_kernel, [((NY * BLK, wide), F32)])(routed, shared)
    got = swap(mid.astype(F16).reshape(NY, BLK, wide), "y")
    pre = jnp.sum(got.astype(F32), axis=0)
    (grads,) = call(hidden_kernel, [((NY, BLK, wide), BF)])(pre, recv)
    own = swap(grads, "y").reshape(NY * BLK, wide)
    main, hid = call(
        pack_kernel, [((NX, NY * (BLK + 1), 2 * HID), BF), ((NY * SLOTS, HID), BF)]
    )(own)
    main = swap(main, "x")
    shared_grad, back = call(
        back_kernel, [((n, feats), F32), ((NC, NZ, 4 * BLK, feats), BF)]
    )(main, tok, cot, wg, wu, sg, su)
    back = swap(back, "core")
    (back,) = call(core_kernel, [((NZ, 5 * BLK, feats), BF)])(back)
    hid, back = lax.optimization_barrier((hid, back))
    turned = {k: turn(hid, k) for k in SHIFTS}
    back = swap(back, "z")
    grad_g, grad_u = call(
        weights_kernel, [struct((2, feats, HID), F32), struct((2, feats, HID), F32)]
    )(main, flat)
    (grad_d,) = call(down_kernel, [struct((2, HID, feats), F32)])(
        hid, turned[1], turned[2], turned[3], flat
    )
    grad_tokens, grad_weights, shared_g, shared_u, shared_d = call(
        final_kernel,
        [
            struct((n, feats), BF),
            struct((2, n), F32),
            struct((BLK, feats), F32),
            struct((BLK, feats), F32),
            struct((BLK, feats), F32),
        ],
    )(back, ids, shared_grad)
    return grad_tokens, grad_weights.T, grad_g, grad_u, grad_d, shared_g.T, shared_u.T, shared_d


def solution(mesh):
    return program(mesh)


def program(mesh):
    ep, tp = ("z", "core"), ("y", "x")
    fine = Mesh(mesh.devices.reshape(NZ, NC, NY, NX), ("z", "core", "y", "x"))
    return jax.shard_map(
        body,
        mesh=fine,
        in_specs=(
            P(ep, tp),
            P(ep, None),
            P(ep, None),
            P(ep, tp),
            P(ep, tp, None),
            P(ep, tp, None),
            P(ep, None, tp),
            P(tp, None),
            P(tp, None),
            P(None, tp),
        ),
        out_specs=(
            P(ep, tp),
            P(ep, None),
            P(ep, tp, None),
            P(ep, tp, None),
            P(ep, None, tp),
            P(tp, ep),
            P(tp, ep),
            P(ep, tp),
        ),
        check_vma=False,
    )
```

```python
import jax
import jax.numpy as jnp
from jax import lax
from jax.experimental import pallas as pl
from jax.experimental.pallas import tpu as pltpu
from jax.sharding import Mesh
from jax.sharding import PartitionSpec as P

BF, F16, F32, I32 = jnp.bfloat16, jnp.float16, jnp.float32, jnp.int32
NZ, NC, NY, NX = 16, 2, 8, 4
NEP, NTP = NZ * NC, NY * NX
CAP, BLK = 5, 16
SLOTS = 2 * CAP
SHR = 4
USED = SLOTS + SHR
PACK = NC * (SLOTS + 2)
HID = 512
SCALE_X, SCALE_Y = 256.0, 64.0

SHIFTS = (1, 3, 2)


def iota(shape, dim):
    return lax.broadcasted_iota(I32, shape, dim)


def nn(a, b):
    return jnp.dot(a, b, preferred_element_type=F32)


def nt(a, b):
    return lax.dot_general(a, b, (((1,), (1,)), ((), ())), preferred_element_type=F32)


def tn(a, b):
    return lax.dot_general(a, b, (((0,), (0,)), ((), ())), preferred_element_type=F32)


def onehot(cond):
    return jnp.where(cond, 1.0, 0.0).astype(BF)


def call(kernel, outs, space=pltpu.VMEM, scratch=()):
    def place(o):
        return o if isinstance(o, jax.ShapeDtypeStruct) else pltpu.VMEM(*o)

    outs = [place(o) for o in outs]

    def run(*args):
        return pl.pallas_call(
            kernel,
            out_shape=outs,
            in_specs=[pl.BlockSpec(memory_space=space)] * len(args),
            out_specs=[pl.BlockSpec(memory_space=pltpu.VMEM)] * len(outs),
            scratch_shapes=scratch,
            compiler_params=pltpu.CompilerParams(vmem_limit_bytes=16 << 20),
        )(*[pltpu.with_memory_space_constraint(a, space) for a in args])

    return run


def struct(shape, dtype):
    return jax.ShapeDtypeStruct(shape, dtype)


def route_kernel(*refs):
    sources, (send, ids), kept = refs[:10], refs[10:12], refs[12:20]
    routes, weights, sems = refs[20:]
    tok, cot = kept[:2]
    copies = [
        pltpu.make_async_copy(a, b, sems.at[k])
        for k, (a, b) in enumerate(zip(sources, (routes, weights, *kept)))
    ]
    for copy in copies:
        copy.start()
    for copy in copies[:4]:
        copy.wait()
    n = tok.shape[0]
    r0, r1 = routes[0:1, :], routes[1:2, :]
    names = iota((NEP * 2, n), 0)
    f0, f1 = jnp.where(r0 == names, 1.0, 0.0), jnp.where(r1 == names, 1.0, 0.0)
    earlier = onehot(iota((n, n), 0) < iota((n, n), 1))
    c0 = nn(f0.astype(BF), earlier)
    c1 = nn(f1.astype(BF), earlier) + jnp.sum(f0, axis=1, keepdims=True)
    rank0 = jnp.sum(c0 * f0, axis=0, keepdims=True).astype(I32)
    rank1 = jnp.sum(c1 * f1, axis=0, keepdims=True).astype(I32)
    row0 = (r0 >> 1) * BLK + (r0 & 1) * CAP + rank0
    row1 = (r1 >> 1) * BLK + (r1 & 1) * CAP + rank1
    ids[0:1, :] = row0
    ids[1:2, :] = row1
    tall = iota((NEP * BLK, n), 0)
    places = onehot((row0 == tall) | (row1 == tall))
    send[:, 128:] = nn(places, cot[...]).astype(BF)
    gates = weights[...].astype(BF).astype(F32)
    data = nn(places, tok[...])
    lane = iota((n, n), 0)
    for row, k in ((row0, 0), (row1, 1)):
        at = jnp.where((row >> 4) * BLK + SLOTS == tall, gates[k : k + 1, :], 0.0).astype(BF)
        data = data + nt(at, onehot(lane == (row & 15)))
    send[:, :128] = data.astype(BF)
    for copy in copies[4:]:
        copy.wait()


def split_rows(r, size):
    if size == USED:
        x = (r * 293) >> 15
        rest = r - x * (NY * USED)
        y = (rest * 293) >> 12
    else:
        x = (r * 205) >> 14
        rest = r - x * (NY * SLOTS)
        y = (rest * 205) >> 11
    return x, y, rest - y * size


def shared_kernel(tok, cot, sg, su, sd, *outs):
    me = lax.axis_index("x")
    r = iota((NTP * SHR, 1), 0)
    s = ((r >> 2) & (NY - 1)) * NX + (((r >> 5) + me) & (NX - 1))
    pick = onehot(s * SHR + (r & 3) == iota((NTP * SHR, 128), 1))
    t = nn(pick, tok[...]).astype(BF)
    c = nn(pick, cot[...]).astype(BF)
    rows = NY * SHR
    for j, part in enumerate((nn(t, sg[...]), nn(t, su[...]), nt(c, sd[...]))):
        for k in range(NX):
            outs[k][:, j * HID : j * HID + HID] = part[k * rows : k * rows + rows] * SCALE_X


def partial_kernel(recv, wg, wu, wd, out):
    x, y, q = split_rows(iota((NTP * SLOTS, 1), 0), SLOTS)
    pick = onehot((y * NX + x) * BLK + q == iota((NTP * SLOTS, NEP * BLK), 1))
    data = nn(pick, recv[...])
    t, c = data[:, :128], data[:, 128:]
    kinds = (q < CAP, q >= CAP)
    tcat = jnp.concatenate([jnp.where(k, t, 0.0).astype(BF) for k in kinds], axis=1)
    ccat = jnp.concatenate([jnp.where(k, c, 0.0).astype(BF) for k in kinds], axis=1)
    wgc = jnp.concatenate([wg[0], wg[1]], axis=0)
    wuc = jnp.concatenate([wu[0], wu[1]], axis=0)
    wdc = jnp.concatenate([wd[0], wd[1]], axis=1)
    out[:, :HID] = nn(tcat, wgc) * SCALE_X
    out[:, HID : 2 * HID] = nn(tcat, wuc) * SCALE_X
    out[:, 2 * HID :] = nt(ccat, wdc) * SCALE_X


def merge_kernel(routed, shared, out):
    for y in range(NY):
        at = y * BLK
        out[at : at + SLOTS] = routed[y * SLOTS : y * SLOTS + SLOTS] * (SCALE_Y / SCALE_X)
        out[at + SLOTS : at + USED] = shared[y * SHR : y * SHR + SHR] * (SCALE_Y / SCALE_X)
        out[at + USED : at + BLK] = jnp.zeros((BLK - USED, out.shape[1]), F32)


def hidden_kernel(got, recv, out):
    t = lax.axis_index("y") * NX + lax.axis_index("x")
    pre = got[...] * (1.0 / SCALE_Y)
    gate, up, back = pre[:, :HID], pre[:, HID : 2 * HID], pre[:, 2 * HID :]
    q = iota((BLK, 1), 0)
    lane = iota((BLK, 128), 1)
    block = recv[t, :, :128].astype(F32)
    grow = jnp.sum(jnp.where(iota((BLK, 128), 0) == SLOTS, block, 0.0), axis=0, keepdims=True)
    gcol = jnp.sum(jnp.where(lane == iota((BLK, 128), 0), grow, 0.0), axis=1, keepdims=True)
    scale = jnp.where(q < SLOTS, gcol, 1.0)
    logistic = jax.nn.sigmoid(gate)
    product = gate * logistic * up
    grad_act = scale * back
    gate_grad = (grad_act * up * logistic * (1.0 + gate * (1.0 - logistic))).astype(BF)
    up_grad = (grad_act * gate * logistic).astype(BF)
    hidden = (scale * product).astype(BF)
    dg = jnp.sum(back * product, axis=1, keepdims=True)
    lane_h = iota((BLK, HID), 1)
    row_h = iota((BLK, HID), 0)
    line = jnp.sum(jnp.where(lane_h == row_h, dg, 0.0), axis=0, keepdims=True)
    high = line.astype(BF).astype(F32)
    extra = jnp.where(row_h == USED, high, line - high)
    gate_grad = jnp.where(row_h >= USED, extra, gate_grad.astype(F32)).astype(BF)
    for k in range(NY):
        out[k, :, :HID] = gate_grad
        out[k, :, HID : 2 * HID] = up_grad
        out[k, :, 2 * HID :] = hidden


def pack_kernel(own, main, hid):
    data = own[:, : 2 * HID]
    hidden = own[:, 2 * HID :]
    r = iota((NY * USED, 1), 0)
    _, y, q = split_rows(r, USED)
    grads = nn(onehot(y * BLK + q == iota((NY * USED, NY * BLK), 1)), data).astype(BF)
    j = iota((BLK, 1), 0)
    lane = iota((BLK, NY * BLK), 1)
    left = nn(onehot((j >> 2) * BLK + SLOTS + (j & 3) == lane), hidden)
    right = nn(onehot(((j >> 2) + 4) * BLK + SLOTS + (j & 3) == lane), hidden)
    row = iota((NY, 1), 0) * BLK + USED
    lane = iota((NY, NY * BLK), 1)
    high = nn(onehot(row == lane), data[:, :128])
    low = nn(onehot(row + 1 == lane), data[:, :128])
    rest = jnp.zeros((NY, 2 * HID - 256), F32)
    shared = jnp.concatenate([left, right], axis=1).astype(BF)
    lines = jnp.concatenate([high, low, rest], axis=1).astype(BF)
    for k in range(NX):
        main[k, : NY * USED] = grads
        main[k, NY * USED : NY * BLK] = shared
        main[k, NY * BLK :] = lines
    _, y, q = split_rows(iota((NY * SLOTS, 1), 0), SLOTS)
    hid[...] = nn(onehot(y * BLK + q == iota((NY * SLOTS, NY * BLK), 1)), hidden).astype(BF)


def back_kernel(main, tok, cot, wg, wu, sg, su, shared_grad, keep, send):
    me = lax.axis_index("core")
    n = tok.shape[0]
    rows, total = NY * USED, NTP * USED
    grads = jnp.concatenate([main[x, :rows] for x in range(NX)], axis=0)
    hidden = jnp.concatenate([main[x, rows : NY * BLK] for x in range(NX)], axis=0)
    lines = jnp.concatenate([main[x, NY * BLK :, :256] for x in range(NX)], axis=0)
    token = iota((n, 1), 0)
    y, x, t = token >> 4, (token >> 2) & 3, token & 3
    pick = onehot(x * rows + y * USED + SLOTS + t == iota((n, total), 1))
    shared = nn(pick, grads).astype(BF)
    j = y * SHR + t
    place = x * BLK + (j & 15)
    lane = iota((n, NX * BLK), 1)
    near = onehot((j < BLK) & (place == lane))
    far = onehot((j >= BLK) & (place == lane))
    shared_hidden = (nn(near, hidden[:, :HID]) + nn(far, hidden[:, HID:])).astype(BF)
    shared_grad[...] = nt(shared[:, :HID], sg[...]) + nt(shared[:, HID:], su[...])
    wt = tn(shared, tok[...]).astype(BF)
    wdn = tn(shared_hidden, cot[...]).astype(BF)
    gg, gu = grads[:, :HID], grads[:, HID:]
    d0 = nt(gg, wg[0]) + nt(gu, wu[0])
    d1 = nt(gg, wg[1]) + nt(gu, wu[1])
    _, _, q = split_rows(iota((total, 1), 0), USED)
    slots = jnp.where(q < CAP, d0, d1).astype(BF)
    o = iota((NEP * BLK, 1), 0)
    q, d = o & 15, o >> 4
    want = jnp.where(q < SLOTS, (d & 3) * rows + (d >> 2) * USED + q, -1)
    back = nn(onehot(want == iota((NEP * BLK, total), 1)), slots)
    source = (d & 3) * NY + (d >> 2)
    lane = iota((NEP * BLK, NTP), 1)
    back = back + nn(onehot((q == USED) & (source == lane)), lines[:, :128])
    back = back + nn(onehot((q == USED + 1) & (source == lane)), lines[:, 128:])
    back = back.astype(BF)
    parts = (back, wt[:HID], wt[HID:], wdn)
    for z in range(NZ):
        for j, part in enumerate(parts):
            a = part[2 * z * BLK : (2 * z + 1) * BLK]
            b = part[(2 * z + 1) * BLK : (2 * z + 2) * BLK]
            at = pl.ds(j * BLK, BLK)
            keep[z, at] = jnp.where(me == 0, a, b)
            send[z, at] = jnp.where(me == 0, b, a)


def weights_kernel(main, recv, og, ou):
    rows, total = NY * USED, NTP * USED
    grads = jnp.concatenate([main[x, :rows] for x in range(NX)], axis=0)
    x, y, q = split_rows(iota((total, 1), 0), USED)
    place = (y * NX + x) * BLK + q
    lane = iota((total, NEP * BLK), 1)
    data = recv[:, :128]
    t0 = nn(onehot((q < CAP) & (place == lane)), data).astype(BF)
    t1 = nn(onehot((q >= CAP) & (q < SLOTS) & (place == lane)), data).astype(BF)
    tcat = jnp.concatenate([t0, t1], axis=1)
    g = tn(tcat, grads[:, :HID])
    og[0], og[1] = g[:128], g[128:]
    u = tn(tcat, grads[:, HID:])
    ou[0], ou[1] = u[:128], u[128:]


def down_kernel(h0, h1, h2, h3, recv, od):
    me = lax.axis_index("x")
    hidden = jnp.concatenate([h0[...], h1[...], h2[...], h3[...]], axis=0)
    k, y, q = split_rows(iota((NTP * SLOTS, 1), 0), SLOTS)
    place = (y * NX + ((me - k) & (NX - 1))) * BLK + q
    lane = iota((NTP * SLOTS, NEP * BLK), 1)
    data = recv[:, 128:]
    c0 = nn(onehot((q < CAP) & (place == lane)), data).astype(BF)
    c1 = nn(onehot((q >= CAP) & (place == lane)), data).astype(BF)
    d = tn(hidden, jnp.concatenate([c0, c1], axis=1))
    od[0], od[1] = d[:, :128], d[:, 128:]


def core_kernel(kept, got, out):
    me = lax.axis_index("core")
    for z in range(NZ):
        mine, other = kept[z].astype(F32), got[z].astype(F32)
        near, far = mine[:BLK], other[:BLK]
        first, second = jnp.where(me == 0, near, far), jnp.where(me == 0, far, near)
        out[z, :PACK] = jnp.concatenate(
            [first[:SLOTS], second[:SLOTS], first[USED:], second[USED:]], axis=0
        ).astype(BF)
        out[z, PACK:] = (mine[BLK:] + other[BLK:]).astype(BF)


def final_kernel(got, ids, shared_grad, grad_tokens, grad_weights, og, ou, od):
    n = ids.shape[1]
    row0, row1 = ids[0:1, :], ids[1:2, :]
    back = jnp.concatenate([got[z, :PACK] for z in range(NZ)], axis=0)
    tall = iota((NZ * PACK, n), 0)
    lane = iota((n, n), 0)
    places = False
    for row, k in ((row0, 0), (row1, 1)):
        z, c, q = row >> 5, (row >> 4) & 1, row & 15
        places = places | (z * PACK + c * SLOTS + q == tall)
        base = z * PACK + NC * SLOTS + 2 * c
        line = tn(back, onehot((tall == base) | (tall == base + 1)))
        grad_weights[k : k + 1, :] = jnp.sum(
            jnp.where(lane == q, line, 0.0), axis=0, keepdims=True
        )
    grad_tokens[...] = (tn(onehot(places), back) + shared_grad[...]).astype(BF)
    total = got[0, PACK:].astype(F32)
    for z in range(1, NZ):
        total = total + got[z, PACK:].astype(F32)
    og[...] = total[:BLK]
    ou[...] = total[BLK : 2 * BLK]
    od[...] = total[2 * BLK :]


def swap(array, axis):
    return lax.all_to_all(array, axis, 0, 0, tiled=True)


def turn(array, shift):
    return lax.ppermute(array, "x", [(i, (i + shift) % NX) for i in range(NX)])


def body(tok, routes, weights, cot, wg, wu, wd, sg, su, sd):
    n, feats = tok.shape
    wide = 3 * HID
    params = (tok, cot, wg, wu, wd, sg, su, sd)
    send, ids, *params = call(
        route_kernel,
        [((NEP * BLK, 2 * feats), BF), ((2, n), I32)] + [(p.shape, BF) for p in params],
        space=pltpu.HBM,
        scratch=[
            pltpu.VMEM((2, n), I32),
            pltpu.VMEM((2, n), F32),
            pltpu.SemaphoreType.DMA((10,)),
        ],
    )(routes.T, weights.T, *params)
    tok, cot, wg, wu, wd, sg, su, sd = params
    recv = swap(send.reshape(NEP, BLK, 2 * feats), ("z", "core"))
    shared = call(shared_kernel, [((NY * SHR, wide), F32)] * NX)(tok, cot, sg, su, sd)
    moved = [turn(shared[k].astype(F16), k).astype(F32) for k in SHIFTS]
    shared = sum(moved, shared[0])
    recv, shared = lax.optimization_barrier((recv, shared))
    flat = recv.reshape(NEP * BLK, 2 * feats)
    (part,) = call(partial_kernel, [((NTP * SLOTS, wide), F32)])(flat, wg, wu, wd)
    got = swap(part.astype(F16).reshape(NX, NY * SLOTS, wide), "x")
    routed = jnp.sum(got.astype(F32), axis=0)
    (mid,) = call(merge_kernel, [((NY * BLK, wide), F32)])(routed, shared)
    got = swap(mid.astype(F16).reshape(NY, BLK, wide), "y")
    pre = jnp.sum(got.astype(F32), axis=0)
    (grads,) = call(hidden_kernel, [((NY, BLK, wide), BF)])(pre, recv)
    own = swap(grads, "y").reshape(NY * BLK, wide)
    main, hid = call(
        pack_kernel, [((NX, NY * (BLK + 1), 2 * HID), BF), ((NY * SLOTS, HID), BF)]
    )(own)
    main = swap(main, "x")
    halves = ((NZ, 4 * BLK, feats), BF)
    shared_grad, keep, give = call(back_kernel, [((n, feats), F32), halves, halves])(main, tok, cot, wg, wu, sg, su)
    other = lax.ppermute(give, "core", [(0, 1), (1, 0)])
    (back,) = call(core_kernel, [((NZ, PACK + 3 * BLK, feats), BF)])(keep, other)
    hid, back = lax.optimization_barrier((hid, back))
    turned = {k: turn(hid, k) for k in SHIFTS}
    back = swap(back, "z")
    grad_g, grad_u = call(
        weights_kernel, [struct((2, feats, HID), F32), struct((2, feats, HID), F32)]
    )(main, flat)
    (grad_d,) = call(down_kernel, [struct((2, HID, feats), F32)])(
        hid, turned[1], turned[2], turned[3], flat
    )
    grad_tokens, grad_weights, shared_g, shared_u, shared_d = call(
        final_kernel,
        [
            struct((n, feats), BF),
            struct((2, n), F32),
            struct((BLK, feats), F32),
            struct((BLK, feats), F32),
            struct((BLK, feats), F32),
        ],
    )(back, ids, shared_grad)
    return grad_tokens, grad_weights.T, grad_g, grad_u, grad_d, shared_g.T, shared_u.T, shared_d


def solution(mesh):
    return program(mesh)


def program(mesh):
    ep, tp = ("z", "core"), ("y", "x")
    fine = Mesh(mesh.devices.reshape(NZ, NC, NY, NX), ("z", "core", "y", "x"))
    return jax.shard_map(
        body,
        mesh=fine,
        in_specs=(
            P(ep, tp),
            P(ep, None),
            P(ep, None),
            P(ep, tp),
            P(ep, tp, None),
            P(ep, tp, None),
            P(ep, None, tp),
            P(tp, None),
            P(tp, None),
            P(None, tp),
        ),
        out_specs=(
            P(ep, tp),
            P(ep, None),
            P(ep, tp, None),
            P(ep, tp, None),
            P(ep, None, tp),
            P(tp, ep),
            P(tp, ep),
            P(ep, tp),
        ),
        check_vma=False,
    )
```

```python
import jax
import jax.numpy as jnp
from jax import lax
from jax.experimental import pallas as pl
from jax.experimental.pallas import tpu as pltpu
from jax.sharding import Mesh
from jax.sharding import PartitionSpec as P

BF, F16, F32, I32 = jnp.bfloat16, jnp.float16, jnp.float32, jnp.int32
NZ, NC, NY, NX = 16, 2, 8, 4
NEP, NTP = NZ * NC, NY * NX
CAP, BLK = 5, 16
SLOTS = 2 * CAP
SHR = 4
USED = SLOTS + SHR
SENT = 24
PACK = NC * (SLOTS + 2)
HID = 512
SCALE_X, SCALE_Y = 256.0, 64.0

SHIFTS = (2, 3, 1)


def iota(shape, dim):
    return lax.broadcasted_iota(I32, shape, dim)


def nn(a, b):
    return jnp.dot(a, b, preferred_element_type=F32)


def nt(a, b):
    return lax.dot_general(a, b, (((1,), (1,)), ((), ())), preferred_element_type=F32)


def tn(a, b):
    return lax.dot_general(a, b, (((0,), (0,)), ((), ())), preferred_element_type=F32)


def onehot(cond):
    return jnp.where(cond, 1.0, 0.0).astype(BF)


def call(kernel, outs, space=pltpu.VMEM, scratch=()):
    def place(o):
        return o if isinstance(o, jax.ShapeDtypeStruct) else pltpu.VMEM(*o)

    outs = [place(o) for o in outs]

    def run(*args):
        return pl.pallas_call(
            kernel,
            out_shape=outs,
            in_specs=[pl.BlockSpec(memory_space=space)] * len(args),
            out_specs=[pl.BlockSpec(memory_space=pltpu.VMEM)] * len(outs),
            scratch_shapes=scratch,
            compiler_params=pltpu.CompilerParams(vmem_limit_bytes=16 << 20),
        )(*[pltpu.with_memory_space_constraint(a, space) for a in args])

    return run


def struct(shape, dtype):
    return jax.ShapeDtypeStruct(shape, dtype)


def route_kernel(*refs):
    sources, (send, ids), kept = refs[:10], refs[10:12], refs[12:20]
    routes, weights, sems = refs[20:]
    tok, cot = kept[:2]
    copies = [
        pltpu.make_async_copy(a, b, sems.at[k])
        for k, (a, b) in enumerate(zip(sources, (routes, weights, *kept)))
    ]
    for copy in copies:
        copy.start()
    for copy in copies[:4]:
        copy.wait()
    n = tok.shape[0]
    r0, r1 = routes[0:1, :], routes[1:2, :]
    names = iota((NEP * 2, n), 0)
    f0, f1 = jnp.where(r0 == names, 1.0, 0.0), jnp.where(r1 == names, 1.0, 0.0)
    earlier = onehot(iota((n, n), 0) < iota((n, n), 1))
    c0 = nn(f0.astype(BF), earlier)
    c1 = nn(f1.astype(BF), earlier) + jnp.sum(f0, axis=1, keepdims=True)
    rank0 = jnp.sum(c0 * f0, axis=0, keepdims=True).astype(I32)
    rank1 = jnp.sum(c1 * f1, axis=0, keepdims=True).astype(I32)
    row0 = (r0 >> 1) * BLK + (r0 & 1) * CAP + rank0
    row1 = (r1 >> 1) * BLK + (r1 & 1) * CAP + rank1
    ids[0:1, :] = row0
    ids[1:2, :] = row1
    tall = iota((NEP * SENT, n), 0)
    spot0, spot1 = (row0 >> 4) * SENT + (row0 & 15), (row1 >> 4) * SENT + (row1 & 15)
    data = nn(onehot((spot0 == tall) | (spot1 == tall)), tok[...])
    data = data + nn(onehot((spot0 + SLOTS == tall) | (spot1 + SLOTS == tall)), cot[...])
    gates = weights[...].astype(BF).astype(F32)
    lane = iota((n, n), 0)
    for row, k in ((row0, 0), (row1, 1)):
        line = (row >> 4) * SENT + 2 * SLOTS
        at = jnp.where(line == tall, gates[k : k + 1, :], 0.0).astype(BF)
        data = data + nt(at, onehot(lane == (row & 15)))
    send[...] = data.astype(BF)
    for copy in copies[4:]:
        copy.wait()


def split_rows(r, size):
    if size == USED:
        x = (r * 293) >> 15
        rest = r - x * (NY * USED)
        y = (rest * 293) >> 12
    else:
        x = (r * 205) >> 14
        rest = r - x * (NY * SLOTS)
        y = (rest * 205) >> 11
    return x, y, rest - y * size


def shared_kernel(tok, cot, sg, su, sd, *outs):
    me = lax.axis_index("x")
    r = iota((NTP * SHR, 1), 0)
    s = ((r >> 2) & (NY - 1)) * NX + (((r >> 5) + me) & (NX - 1))
    pick = onehot(s * SHR + (r & 3) == iota((NTP * SHR, 128), 1))
    t = nn(pick, tok[...]).astype(BF)
    c = nn(pick, cot[...]).astype(BF)
    rows = NY * SHR
    for j, part in enumerate((nn(t, sg[...]), nn(t, su[...]), nt(c, sd[...]))):
        for k in range(NX):
            outs[k][:, j * HID : j * HID + HID] = part[k * rows : k * rows + rows] * SCALE_X


def partial_kernel(recv, wg, wu, wd, out):
    x, y, q = split_rows(iota((NTP * SLOTS, 1), 0), SLOTS)
    place = (y * NX + x) * SENT + q
    lane = iota((NTP * SLOTS, NEP * SENT), 1)
    t = nn(onehot(place == lane), recv[...])
    c = nn(onehot(place + SLOTS == lane), recv[...])
    kinds = (q < CAP, q >= CAP)
    tcat = jnp.concatenate([jnp.where(k, t, 0.0).astype(BF) for k in kinds], axis=1)
    ccat = jnp.concatenate([jnp.where(k, c, 0.0).astype(BF) for k in kinds], axis=1)
    wgc = jnp.concatenate([wg[0], wg[1]], axis=0)
    wuc = jnp.concatenate([wu[0], wu[1]], axis=0)
    wdc = jnp.concatenate([wd[0], wd[1]], axis=1)
    out[:, :HID] = nn(tcat, wgc) * SCALE_X
    out[:, HID : 2 * HID] = nn(tcat, wuc) * SCALE_X
    out[:, 2 * HID :] = nt(ccat, wdc) * SCALE_X


def merge_kernel(routed, shared, out):
    for y in range(NY):
        at = y * BLK
        out[at : at + SLOTS] = routed[y * SLOTS : y * SLOTS + SLOTS] * (SCALE_Y / SCALE_X)
        out[at + SLOTS : at + USED] = shared[y * SHR : y * SHR + SHR] * (SCALE_Y / SCALE_X)
        out[at + USED : at + BLK] = jnp.zeros((BLK - USED, out.shape[1]), F32)


def hidden_kernel(got, recv, out):
    t = lax.axis_index("y") * NX + lax.axis_index("x")
    pre = got[...] * (1.0 / SCALE_Y)
    gate, up, back = pre[:, :HID], pre[:, HID : 2 * HID], pre[:, 2 * HID :]
    q = iota((BLK, 1), 0)
    lane = iota((BLK, 128), 1)
    block = recv[t].astype(F32)
    line = iota((SENT, 128), 0) == 2 * SLOTS
    grow = jnp.sum(jnp.where(line, block, 0.0), axis=0, keepdims=True)
    gcol = jnp.sum(jnp.where(lane == iota((BLK, 128), 0), grow, 0.0), axis=1, keepdims=True)
    scale = jnp.where(q < SLOTS, gcol, 1.0)
    logistic = jax.nn.sigmoid(gate)
    product = gate * logistic * up
    grad_act = scale * back
    gate_grad = (grad_act * up * logistic * (1.0 + gate * (1.0 - logistic))).astype(BF)
    up_grad = (grad_act * gate * logistic).astype(BF)
    hidden = (scale * product).astype(BF)
    dg = jnp.sum(back * product, axis=1, keepdims=True)
    lane_h = iota((BLK, HID), 1)
    row_h = iota((BLK, HID), 0)
    line = jnp.sum(jnp.where(lane_h == row_h, dg, 0.0), axis=0, keepdims=True)
    high = line.astype(BF).astype(F32)
    extra = jnp.where(row_h == USED, high, line - high)
    gate_grad = jnp.where(row_h >= USED, extra, gate_grad.astype(F32)).astype(BF)
    for k in range(NY):
        out[k, :, :HID] = gate_grad
        out[k, :, HID : 2 * HID] = up_grad
        out[k, :, 2 * HID :] = hidden


def pack_kernel(own, main, hid):
    data = own[:, : 2 * HID]
    hidden = own[:, 2 * HID :]
    r = iota((NY * USED, 1), 0)
    _, y, q = split_rows(r, USED)
    grads = nn(onehot(y * BLK + q == iota((NY * USED, NY * BLK), 1)), data).astype(BF)
    j = iota((BLK, 1), 0)
    lane = iota((BLK, NY * BLK), 1)
    left = nn(onehot((j >> 2) * BLK + SLOTS + (j & 3) == lane), hidden)
    right = nn(onehot(((j >> 2) + 4) * BLK + SLOTS + (j & 3) == lane), hidden)
    row = iota((NY, 1), 0) * BLK + USED
    lane = iota((NY, NY * BLK), 1)
    high = nn(onehot(row == lane), data[:, :128])
    low = nn(onehot(row + 1 == lane), data[:, :128])
    rest = jnp.zeros((NY, 2 * HID - 256), F32)
    shared = jnp.concatenate([left, right], axis=1).astype(BF)
    lines = jnp.concatenate([high, low, rest], axis=1).astype(BF)
    for k in range(NX):
        main[k, : NY * USED] = grads
        main[k, NY * USED : NY * BLK] = shared
        main[k, NY * BLK :] = lines
    _, y, q = split_rows(iota((NY * SLOTS, 1), 0), SLOTS)
    hid[...] = nn(onehot(y * BLK + q == iota((NY * SLOTS, NY * BLK), 1)), hidden).astype(BF)


def back_kernel(main, tok, cot, wg, wu, sg, su, shared_grad, keep, send):
    me = lax.axis_index("core")
    n = tok.shape[0]
    rows, total = NY * USED, NTP * USED
    grads = jnp.concatenate([main[x, :rows] for x in range(NX)], axis=0)
    hidden = jnp.concatenate([main[x, rows : NY * BLK] for x in range(NX)], axis=0)
    lines = jnp.concatenate([main[x, NY * BLK :, :256] for x in range(NX)], axis=0)
    token = iota((n, 1), 0)
    y, x, t = token >> 4, (token >> 2) & 3, token & 3
    pick = onehot(x * rows + y * USED + SLOTS + t == iota((n, total), 1))
    shared = nn(pick, grads).astype(BF)
    j = y * SHR + t
    place = x * BLK + (j & 15)
    lane = iota((n, NX * BLK), 1)
    near = onehot((j < BLK) & (place == lane))
    far = onehot((j >= BLK) & (place == lane))
    shared_hidden = (nn(near, hidden[:, :HID]) + nn(far, hidden[:, HID:])).astype(BF)
    shared_grad[...] = nt(shared[:, :HID], sg[...]) + nt(shared[:, HID:], su[...])
    wt = tn(shared, tok[...]).astype(BF)
    wdn = tn(shared_hidden, cot[...]).astype(BF)
    gg, gu = grads[:, :HID], grads[:, HID:]
    d0 = nt(gg, wg[0]) + nt(gu, wu[0])
    d1 = nt(gg, wg[1]) + nt(gu, wu[1])
    _, _, q = split_rows(iota((total, 1), 0), USED)
    slots = jnp.where(q < CAP, d0, d1).astype(BF)
    o = iota((NEP * BLK, 1), 0)
    q, d = o & 15, o >> 4
    want = jnp.where(q < SLOTS, (d & 3) * rows + (d >> 2) * USED + q, -1)
    back = nn(onehot(want == iota((NEP * BLK, total), 1)), slots)
    source = (d & 3) * NY + (d >> 2)
    lane = iota((NEP * BLK, NTP), 1)
    back = back + nn(onehot((q == USED) & (source == lane)), lines[:, :128])
    back = back + nn(onehot((q == USED + 1) & (source == lane)), lines[:, 128:])
    back = back.astype(BF)
    parts = (back, wt[:HID], wt[HID:], wdn)
    for z in range(NZ):
        for j, part in enumerate(parts):
            a = part[2 * z * BLK : (2 * z + 1) * BLK]
            b = part[(2 * z + 1) * BLK : (2 * z + 2) * BLK]
            at = pl.ds(j * BLK, BLK)
            keep[z, at] = jnp.where(me == 0, a, b)
            send[z, at] = jnp.where(me == 0, b, a)


def weights_kernel(main, recv, og, ou):
    rows, total = NY * USED, NTP * USED
    grads = jnp.concatenate([main[x, :rows] for x in range(NX)], axis=0)
    x, y, q = split_rows(iota((total, 1), 0), USED)
    place = (y * NX + x) * SENT + q
    lane = iota((total, NEP * SENT), 1)
    data = recv[...]
    t0 = nn(onehot((q < CAP) & (place == lane)), data).astype(BF)
    t1 = nn(onehot((q >= CAP) & (q < SLOTS) & (place == lane)), data).astype(BF)
    tcat = jnp.concatenate([t0, t1], axis=1)
    g = tn(tcat, grads[:, :HID])
    og[0], og[1] = g[:128], g[128:]
    u = tn(tcat, grads[:, HID:])
    ou[0], ou[1] = u[:128], u[128:]


def down_kernel(h0, h1, h2, h3, recv, od):
    me = lax.axis_index("x")
    hidden = jnp.concatenate([h0[...], h1[...], h2[...], h3[...]], axis=0)
    k, y, q = split_rows(iota((NTP * SLOTS, 1), 0), SLOTS)
    place = (y * NX + ((me - k) & (NX - 1))) * SENT + SLOTS + q
    lane = iota((NTP * SLOTS, NEP * SENT), 1)
    data = recv[...]
    c0 = nn(onehot((q < CAP) & (place == lane)), data).astype(BF)
    c1 = nn(onehot((q >= CAP) & (place == lane)), data).astype(BF)
    d = tn(hidden, jnp.concatenate([c0, c1], axis=1))
    od[0], od[1] = d[:, :128], d[:, 128:]


def core_kernel(kept, got, out):
    me = lax.axis_index("core")
    for z in range(NZ):
        mine, other = kept[z].astype(F32), got[z].astype(F32)
        near, far = mine[:BLK], other[:BLK]
        first, second = jnp.where(me == 0, near, far), jnp.where(me == 0, far, near)
        out[z, :PACK] = jnp.concatenate(
            [first[:SLOTS], second[:SLOTS], first[USED:], second[USED:]], axis=0
        ).astype(BF)
        out[z, PACK:] = (mine[BLK:] + other[BLK:]).astype(BF)


def final_kernel(got, ids, shared_grad, grad_tokens, grad_weights, og, ou, od):
    n = ids.shape[1]
    row0, row1 = ids[0:1, :], ids[1:2, :]
    back = jnp.concatenate([got[z, :PACK] for z in range(NZ)], axis=0)
    tall = iota((NZ * PACK, n), 0)
    lane = iota((n, n), 0)
    places = False
    for row, k in ((row0, 0), (row1, 1)):
        z, c, q = row >> 5, (row >> 4) & 1, row & 15
        places = places | (z * PACK + c * SLOTS + q == tall)
        base = z * PACK + NC * SLOTS + 2 * c
        line = tn(back, onehot((tall == base) | (tall == base + 1)))
        grad_weights[k : k + 1, :] = jnp.sum(
            jnp.where(lane == q, line, 0.0), axis=0, keepdims=True
        )
    grad_tokens[...] = (tn(onehot(places), back) + shared_grad[...]).astype(BF)
    total = got[0, PACK:].astype(F32)
    for z in range(1, NZ):
        total = total + got[z, PACK:].astype(F32)
    og[...] = total[:BLK]
    ou[...] = total[BLK : 2 * BLK]
    od[...] = total[2 * BLK :]


def swap(array, axis):
    return lax.all_to_all(array, axis, 0, 0, tiled=True)


def turn(array, shift):
    return lax.ppermute(array, "x", [(i, (i + shift) % NX) for i in range(NX)])


def body(tok, routes, weights, cot, wg, wu, wd, sg, su, sd):
    n, feats = tok.shape
    wide = 3 * HID
    params = (tok, cot, wg, wu, wd, sg, su, sd)
    send, ids, *params = call(
        route_kernel,
        [((NEP * SENT, feats), BF), ((2, n), I32)] + [(p.shape, BF) for p in params],
        space=pltpu.HBM,
        scratch=[
            pltpu.VMEM((2, n), I32),
            pltpu.VMEM((2, n), F32),
            pltpu.SemaphoreType.DMA((10,)),
        ],
    )(routes.T, weights.T, *params)
    tok, cot, wg, wu, wd, sg, su, sd = params
    recv = swap(send.reshape(NEP, SENT, feats), ("z", "core"))
    shared = call(shared_kernel, [((NY * SHR, wide), F32)] * NX)(tok, cot, sg, su, sd)
    moved = [turn(shared[k].astype(F16), k).astype(F32) for k in SHIFTS]
    shared = sum(moved, shared[0])
    recv, shared = lax.optimization_barrier((recv, shared))
    flat = recv.reshape(NEP * SENT, feats)
    (part,) = call(partial_kernel, [((NTP * SLOTS, wide), F32)])(flat, wg, wu, wd)
    got = swap(part.astype(F16).reshape(NX, NY * SLOTS, wide), "x")
    routed = jnp.sum(got.astype(F32), axis=0)
    (mid,) = call(merge_kernel, [((NY * BLK, wide), F32)])(routed, shared)
    got = swap(mid.astype(F16).reshape(NY, BLK, wide), "y")
    pre = jnp.sum(got.astype(F32), axis=0)
    (grads,) = call(hidden_kernel, [((NY, BLK, wide), BF)])(pre, recv)
    own = swap(grads, "y").reshape(NY * BLK, wide)
    main, hid = call(
        pack_kernel, [((NX, NY * (BLK + 1), 2 * HID), BF), ((NY * SLOTS, HID), BF)]
    )(own)
    main = swap(main, "x")
    halves = ((NZ, 4 * BLK, feats), BF)
    shared_grad, keep, give = call(back_kernel, [((n, feats), F32), halves, halves])(main, tok, cot, wg, wu, sg, su)
    other = lax.ppermute(give, "core", [(0, 1), (1, 0)])
    (back,) = call(core_kernel, [((NZ, PACK + 3 * BLK, feats), BF)])(keep, other)
    hid, back = lax.optimization_barrier((hid, back))
    turned = {k: turn(hid, k) for k in SHIFTS}
    back = swap(back, "z")
    grad_g, grad_u = call(
        weights_kernel, [struct((2, feats, HID), F32), struct((2, feats, HID), F32)]
    )(main, flat)
    (grad_d,) = call(down_kernel, [struct((2, HID, feats), F32)])(
        hid, turned[1], turned[2], turned[3], flat
    )
    grad_tokens, grad_weights, shared_g, shared_u, shared_d = call(
        final_kernel,
        [
            struct((n, feats), BF),
            struct((2, n), F32),
            struct((BLK, feats), F32),
            struct((BLK, feats), F32),
            struct((BLK, feats), F32),
        ],
    )(back, ids, shared_grad)
    return grad_tokens, grad_weights.T, grad_g, grad_u, grad_d, shared_g.T, shared_u.T, shared_d


def solution(mesh):
    return program(mesh)


def program(mesh):
    ep, tp = ("z", "core"), ("y", "x")
    fine = Mesh(mesh.devices.reshape(NZ, NC, NY, NX), ("z", "core", "y", "x"))
    return jax.shard_map(
        body,
        mesh=fine,
        in_specs=(
            P(ep, tp),
            P(ep, None),
            P(ep, None),
            P(ep, tp),
            P(ep, tp, None),
            P(ep, tp, None),
            P(ep, None, tp),
            P(tp, None),
            P(tp, None),
            P(None, tp),
        ),
        out_specs=(
            P(ep, tp),
            P(ep, None),
            P(ep, tp, None),
            P(ep, tp, None),
            P(ep, None, tp),
            P(tp, ep),
            P(tp, ep),
            P(ep, tp),
        ),
        check_vma=False,
    )
```
